32 devices in a mesh: sp: 8 (over z, y), tp: 4 (over x, core).
Axes of the slice: x: 2, y: 2, z: 4, core: 2. Of those that a mesh axis runs over, the one named last changes fastest.
Arguments:
- latents: bfloat16 [5120, 2048], P('sp'), may hold values from -6 to 6
- cond: float32 [2048], replicated, may hold values from -6 to 6
- ctx_cond: float32 [2048], replicated, may hold values from -6 to 6
- context: bfloat16 [768, 2048], P('sp'), may hold values from -6 to 6
- norm_gain: float32 [2048], replicated, may hold values from 0.1 to 1.9
- shift_weight: bfloat16 [2048, 2048], P('tp'), may hold values from -0.125 to 0.125
- scale_weight: bfloat16 [2048, 2048], P('tp'), may hold values from -0.125 to 0.125
- gate_weight: bfloat16 [2048, 2048], P('tp'), may hold values from -0.125 to 0.125
- q_weight: bfloat16 [2048, 1024], P(None, 'tp'), may hold values from -0.125 to 0.125
- k_weight: bfloat16 [2048, 1024], P(None, 'tp'), may hold values from -0.125 to 0.125
- v_weight: bfloat16 [2048, 1024], P(None, 'tp'), may hold values from -0.125 to 0.125
- out_weight: bfloat16 [1024, 2048], replicated, may hold values from -1.5 to 1.5
- rel_bias: float32 [8, 15, 31], P('tp'), may hold values from 1.5 to 260
Outputs:
- result: bfloat16 [5120, 2048], P(('sp', 'tp'))
The draws below stay inside these ranges and needn't reach their ends.
All inputs are finite; a program needn't handle non-finite values.
Results may differ from the reference program's by a relative error of at most 0.0085.
Values may be sent and summed in bfloat16 or wider, within the bound.
A program may use at most 64 MiB of HBM per device.

```python
import jax
import jax.numpy as jnp
from jax import lax

D = 2048
HEADS = 8
HEAD_DIM = 128
GRID_W = 64
WIN_ROWS = 8
WIN_COLS = 16
CTX = 768
ROWS = 80
TOKENS = 5120
NA_WIDTH = 1024


def draw_rel_bias(key, part):
    base_key = jax.random.fold_in(jax.random.fold_in(key, 4711), 0)
    table = jax.random.uniform(base_key, (HEADS, 2 * WIN_ROWS - 1, 2 * WIN_COLS - 1), jnp.float32, 1.5, 4.5)
    return table.astype(jnp.float32)


def block_scale(own_key, extent, cuts, low, top_value):
    def one(axis_at, parts):
        steps = jax.random.uniform(jax.random.fold_in(jax.random.fold_in(own_key, 6), axis_at), (parts,), jnp.float32, low / len(cuts), top_value / len(cuts))
        return jnp.repeat(jnp.exp(steps), extent[axis_at] // parts).reshape((-1,) + (1,) * (len(extent) - axis_at - 1))

    level = one(*cuts[0])
    for cut in cuts[1:]:
        level = level * one(*cut)
    return level


def noise(stream_key, shape, width, limit, cuts=(), kind=jnp.bfloat16):
    level = block_scale(stream_key, shape, cuts, -0.22, 0.18) if cuts else 1.0
    array = jax.random.normal(stream_key, shape, jnp.float32) * width * level
    return jnp.minimum(jnp.maximum(array, -limit), limit).astype(kind)


def setup_inputs(seed: int = 0) -> dict:
    key_list = jax.random.split(jax.random.key(seed), 14)
    return {
        "latents": noise(key_list[0], (TOKENS, D), 1.0, 6.0, ((0, 8),)),
        "cond": noise(key_list[1], (D,), 1.0, 6.0, (), jnp.float32),
        "ctx_cond": noise(key_list[2], (D,), 1.0, 6.0, (), jnp.float32),
        "context": noise(key_list[3], (CTX, D), 1.0, 6.0, ((0, 8),)),
        "norm_gain": jnp.clip(1.0 + 0.18 * jax.random.normal(key_list[4], (D,), jnp.float32), 0.1, 1.9),
        "shift_weight": noise(key_list[5], (D, D), D ** -0.5, 0.125, ((0, 4),)),
        "scale_weight": noise(key_list[6], (D, D), D ** -0.5, 0.125, ((0, 4),)),
        "gate_weight": noise(key_list[7], (D, D), D ** -0.5, 0.125, ((0, 4),)),
        "q_weight": noise(key_list[8], (D, NA_WIDTH), D ** -0.5, 0.125, ((1, 4),)),
        "k_weight": noise(key_list[9], (D, NA_WIDTH), D ** -0.5, 0.125, ((1, 4),)),
        "v_weight": noise(key_list[10], (D, NA_WIDTH), D ** -0.5, 0.125, ((1, 4),)),
        "out_weight": noise(key_list[11], (NA_WIDTH, D), (max(NA_WIDTH // 64, 1)) ** -0.5, 1.5),
        "rel_bias": draw_rel_bias(jax.random.fold_in(key_list[13], 71), 0),
    }


EPS = 1e-06
NEG_BIG = -1e+30

def modulated_norm(tok_rows, gain, shift_row, scale_row):
    rows_f = tok_rows.astype(jnp.float32)
    inverse = lax.rsqrt(lax.optimization_barrier(jnp.mean(rows_f * rows_f, axis=-1, keepdims=True)) + EPS)
    return (rows_f * inverse * gain * (1.0 + scale_row) + shift_row).astype(jnp.bfloat16)

def column_mask():
    columns = jnp.arange(GRID_W, dtype=jnp.int32)
    first_col = jnp.clip(columns - WIN_COLS // 2, 0, GRID_W - WIN_COLS)
    inside = (columns[None, :] >= first_col[:, None]) & (columns[None, :] < first_col[:, None] + WIN_COLS)
    return jnp.tile(inside, (1, WIN_ROWS))

def grid_bias(bias_table, row_diff):
    row_hot = (row_diff[:, :, None] == jnp.arange(2 * WIN_ROWS - 1, dtype=jnp.int32)[None, None, :]).astype(jnp.float32)
    columns = jnp.arange(GRID_W, dtype=jnp.int32)
    col_diff = jnp.clip(columns[None, :] - columns[:, None], -(WIN_COLS - 1), WIN_COLS - 1) + WIN_COLS - 1
    col_hot = (col_diff[:, :, None] == jnp.arange(2 * WIN_COLS - 1, dtype=jnp.int32)[None, None, :]).astype(jnp.float32)
    middle = jnp.einsum('rai,hij->hraj', row_hot, bias_table.astype(jnp.float32), precision=lax.Precision.HIGHEST)
    spread = jnp.einsum('hraj,qbj->hrqab', middle, col_hot, precision=lax.Precision.HIGHEST)
    return spread.reshape(bias_table.shape[0], row_diff.shape[0], GRID_W, WIN_ROWS * GRID_W)

def attend(query, key_win, val_win, ctx_keys, ctx_vals, bias, inside):
    factor = HEAD_DIM ** (-0.5)
    near_scores = jnp.einsum('rqhd,rkhd->hrqk', query.astype(jnp.float32), key_win.astype(jnp.float32)) * factor + bias
    near_scores = jnp.where(inside, near_scores, NEG_BIG)
    far_scores = jnp.einsum('rqhd,lhd->hrql', query.astype(jnp.float32), ctx_keys.astype(jnp.float32)) * factor
    row_peak = jnp.maximum(lax.optimization_barrier(jnp.max(near_scores, axis=-1, keepdims=True)), lax.optimization_barrier(jnp.max(far_scores, axis=-1, keepdims=True)))
    near_exp = jnp.exp(near_scores - row_peak)
    far_exp = jnp.exp(far_scores - row_peak)
    denominator = lax.optimization_barrier(jnp.sum(near_exp, axis=-1, keepdims=True)) + lax.optimization_barrier(jnp.sum(far_exp, axis=-1, keepdims=True))
    near_w = (near_exp / denominator).astype(jnp.bfloat16)
    far_w = (far_exp / denominator).astype(jnp.bfloat16)
    mixed = jnp.einsum('hrqk,rkhd->rqhd', near_w.astype(jnp.float32), val_win.astype(jnp.float32)) + jnp.einsum('hrql,lhd->rqhd', far_w.astype(jnp.float32), ctx_vals.astype(jnp.float32))
    return mixed.astype(jnp.bfloat16)

def reference(latents, cond, ctx_cond, context, norm_gain, shift_weight, scale_weight, gate_weight, q_weight, k_weight, v_weight, out_weight, rel_bias):
    conds = jnp.stack([cond, ctx_cond])
    active = jax.nn.silu(conds).astype(jnp.bfloat16)
    shifts = jnp.dot(active, shift_weight, preferred_element_type=jnp.float32)
    scales = jnp.dot(active, scale_weight, preferred_element_type=jnp.float32)
    gates = jnp.dot(active[:1], gate_weight, preferred_element_type=jnp.float32)
    h_lat = modulated_norm(latents, norm_gain, shifts[0], scales[0])
    h_ctx = modulated_norm(context, norm_gain, shifts[1], scales[1])
    query = jnp.dot(h_lat, q_weight, preferred_element_type=jnp.float32).astype(jnp.bfloat16)
    keys = jnp.dot(h_lat, k_weight, preferred_element_type=jnp.float32).astype(jnp.bfloat16)
    values = jnp.dot(h_lat, v_weight, preferred_element_type=jnp.float32).astype(jnp.bfloat16)
    ctx_keys = jnp.dot(h_ctx, k_weight, preferred_element_type=jnp.float32).astype(jnp.bfloat16)
    ctx_vals = jnp.dot(h_ctx, v_weight, preferred_element_type=jnp.float32).astype(jnp.bfloat16)
    grid_rows = jnp.arange(ROWS, dtype=jnp.int32)
    first_row = jnp.clip(grid_rows - WIN_ROWS // 2, 0, ROWS - WIN_ROWS)
    offsets = jnp.arange(WIN_ROWS, dtype=jnp.int32)
    row_index = first_row[:, None] + offsets[None, :]
    row_diff = row_index - grid_rows[:, None] + WIN_ROWS - 1
    inside = column_mask()
    query_grid = query.reshape(ROWS, GRID_W, HEADS, HEAD_DIM)
    key_grid = keys.reshape(ROWS, GRID_W, HEADS, HEAD_DIM)
    val_grid = values.reshape(ROWS, GRID_W, HEADS, HEAD_DIM)
    ctx_key3 = ctx_keys.reshape(CTX, HEADS, HEAD_DIM)
    ctx_val3 = ctx_vals.reshape(CTX, HEADS, HEAD_DIM)

    def one_head(head_id):
        query_head = lax.dynamic_slice_in_dim(query_grid, head_id, 1, 2)
        key_head = lax.dynamic_slice_in_dim(key_grid, head_id, 1, 2)[row_index]
        val_head = lax.dynamic_slice_in_dim(val_grid, head_id, 1, 2)[row_index]
        key_head = key_head.reshape(ROWS, WIN_ROWS * GRID_W, 1, HEAD_DIM)
        val_head = val_head.reshape(ROWS, WIN_ROWS * GRID_W, 1, HEAD_DIM)
        ctx_key_head = lax.dynamic_slice_in_dim(ctx_key3, head_id, 1, 1)
        ctx_val_head = lax.dynamic_slice_in_dim(ctx_val3, head_id, 1, 1)
        bias = grid_bias(lax.dynamic_slice_in_dim(rel_bias, head_id, 1, 0), row_diff)
        return attend(query_head, key_head, val_head, ctx_key_head, ctx_val_head, bias, inside)
    head_outs = lax.map(one_head, jnp.arange(HEADS, dtype=jnp.int32))
    attn = jnp.transpose(head_outs[:, :, :, 0], (1, 2, 0, 3)).reshape(TOKENS, NA_WIDTH)
    mixed = jnp.dot(attn, out_weight, preferred_element_type=jnp.float32)
    return (latents.astype(jnp.float32) + gates[0] * mixed).astype(jnp.bfloat16)
```

```python
import functools

import jax
import jax.numpy as jnp
from jax import lax
from jax.experimental import pallas as pl
from jax.experimental.pallas import tpu as pltpu
from jax.sharding import PartitionSpec as P

HEAD_DIM = 128
GRID_W = 64
WIN_ROWS = 8
WIN_COLS = 16
EPS = 1e-06
NEG_BIG = -1e30
F32 = jnp.float32
BF16 = jnp.bfloat16
UP_ROWS = WIN_ROWS // 2
DOWN_ROWS = WIN_ROWS // 2 - 1
PAIR = 2 * GRID_W
KEY_ROWS = WIN_ROWS + 2
KEYS = KEY_ROWS * GRID_W
TABLES = 2 * WIN_ROWS - 2
VMEM_BYTES = 67043328


def dot(a, b):
    return jnp.dot(a, b, preferred_element_type=F32)


def dot_t(a, b):
    return lax.dot_general(a, b, (((1,), (1,)), ((), ())), preferred_element_type=F32)


def wide(x, n):
    if n % HEAD_DIM:
        return x[:, 0:1]
    return jnp.concatenate([x] * (n // HEAD_DIM), axis=1)


def kernel(
    ns, nt, ny,
    cond_h, ctx_cond_h, gain_h, table_h,
    lat_h, ctx_h, wsh_h, wsc_h, wg_h, wq_h, wk_h, wv_h, wo_h,
    own, wo, gates, lat_own,
    lat, ctx, wsh, wsc, wg, wqkv,
    modr, gater, mods, inv, hbuf, ctx_all, kv, q, bias, s_near, s_far, acc, mx, att, lines,
    cond, ctx_cond, gain, table,
    load_sem, mod_s, mod_r, gate_s, gate_r, ctx_s, ctx_r, halo_s, halo_r, head_s, head_r,
):
    sp, tp = lax.axis_index("sp"), lax.axis_index("tp")
    tokens, d = lat.shape
    c_here = ctx.shape[0]
    width = q.shape[1]
    heads = width // HEAD_DIM
    kt = wsh.shape[0]
    rows = tokens // GRID_W
    total_rows = rows * ns
    own_n = tokens // nt
    up_n, down_n = UP_ROWS * GRID_W, DOWN_ROWS * GRID_W
    to_log2 = 1.4426950408889634
    q_scale = HEAD_DIM ** -0.5 * to_log2
    half_d = d // 2
    step = 512

    count = [0]

    def load(s, t):
        c = pltpu.make_async_copy(s, t, load_sem.at[count[0]])
        count[0] += 1
        return c

    small = [load(cond_h, cond), load(ctx_cond_h, ctx_cond), load(gain_h, gain), load(table_h, table)]
    mod_loads = []
    for n0 in range(0, half_d, step):
        mod_loads.append([
            load(s.at[:, pl.ds(k * half_d + n0, step)], t.at[:, pl.ds(k * half_d + n0, step)])
            for k in range(2) for s, t in ((wsh_h, wsh), (wsc_h, wsc))
        ])
    ctx_load, lat_load, wg_load = load(ctx_h, ctx), load(lat_h, lat), load(wg_h, wg)
    wk_load = load(wk_h, wqkv.at[:, pl.ds(0, width)])
    wv_load = load(wv_h, wqkv.at[:, pl.ds(width, width)])
    wq_load = load(wq_h, wqkv.at[:, pl.ds(2 * width, width)])
    wo_load = load(wo_h, wo)
    my_rows = pl.ds(pl.multiple_of(tp * own_n, 16), own_n)
    own_load = load(lat_h.at[my_rows], lat_own)
    for c in small + sum(mod_loads, []) + [ctx_load, lat_load, wg_load, wk_load, wv_load, wq_load, wo_load, own_load]:
        c.start()

    barrier = pltpu.get_barrier_semaphore()

    def greet_tp(o, _):
        pl.semaphore_signal(barrier, inc=1, device_id={"sp": sp, "tp": (tp + o) % nt})
        return 0

    def greet_sp(o, _):
        pl.semaphore_signal(barrier, inc=1, device_id={"sp": (sp + o) % ns, "tp": tp})
        return 0

    lax.fori_loop(1, nt, greet_tp, 0)
    lax.fori_loop(1, ns, greet_sp, 0)

    for c in small:
        c.wait()

    start = pl.multiple_of(tp * kt, 128)
    row = lax.broadcasted_iota(jnp.int32, (8, kt), 0)

    def silu(ref):
        v = ref[:, pl.ds(start, kt)]
        return jnp.broadcast_to(v / (1.0 + jnp.exp(-v)), (8, kt))

    row0_act = silu(cond)
    mixed_act = jnp.where(row % 2 == 0, row0_act, silu(ctx_cond))

    def only(a, keep):
        return jnp.where(keep, a, 0.0).astype(BF16)

    a_sh = [only(mixed_act, (row // 2) == 2 * k) for k in range(2)]
    a_sc = [only(mixed_act, (row // 2) == 2 * k + 1) for k in range(2)]
    for i, n0 in enumerate(range(0, half_d, step)):
        part = jnp.zeros((8, step), F32)
        for k in range(2):
            cols = pl.ds(k * half_d + n0, step)
            mod_loads[i][2 * k].wait()
            part = part + dot(a_sh[k], wsh[:, cols])
            mod_loads[i][2 * k + 1].wait()
            part = part + dot(a_sc[k], wsc[:, cols])
        modr[tp, :, pl.ds(n0, step)] = part
    pl.semaphore_wait(barrier, nt - 1 + ns - 1)

    def tp_copy(buf, s_sem, r_sem, o):
        return pltpu.make_async_remote_copy(
            src_ref=buf.at[tp], dst_ref=buf.at[tp],
            send_sem=s_sem.at[o], recv_sem=r_sem.at[o],
            device_id={"sp": sp, "tp": (tp + o) % nt},
        )

    def start_mod(o, _):
        tp_copy(modr, mod_s, mod_r, o).start()
        return 0

    lax.fori_loop(1, nt, start_mod, 0)

    qc = lax.broadcasted_iota(jnp.int32, (GRID_W, PAIR), 0)
    lane = lax.broadcasted_iota(jnp.int32, (GRID_W, PAIR), 1)
    kc = lane % GRID_W
    first = jnp.clip(qc - WIN_COLS // 2, 0, GRID_W - WIN_COLS)
    inside = (kc >= first) & (kc < first + WIN_COLS)
    lines[...] = jnp.zeros_like(lines)
    lines[:, :, 0:2 * WIN_COLS - 1] = table[...]
    low_row = WIN_ROWS - 1 - WIN_ROWS // 2
    for h in range(heads):
        for i in range(TABLES):
            near_line = jnp.broadcast_to(lines[i, h:h + 1, :], (GRID_W, PAIR))
            next_line = jnp.broadcast_to(lines[i + 1, h:h + 1, :], (GRID_W, PAIR))
            reach = WIN_COLS - 1
            rolled = pltpu.roll(near_line, PAIR - reach, 1, stride=1, stride_axis=0)
            rolled = rolled + pltpu.roll(next_line, GRID_W - reach, 1, stride=1, stride_axis=0)
            both = jnp.where(inside, rolled * to_log2, NEG_BIG)
            bias[h, i] = both
            if i == low_row - 1:
                bias[h, TABLES] = jnp.where(lane >= GRID_W, both, NEG_BIG)
            if i == low_row + WIN_ROWS - 1:
                bias[h, TABLES + 1] = jnp.where(lane < GRID_W, both, NEG_BIG)
        bias[h, TABLES + 2] = jnp.full((GRID_W, PAIR), NEG_BIG, F32)
    mx[...] = jnp.full_like(mx, NEG_BIG)
    acc[...] = jnp.zeros_like(acc)
    n_keys = kv.shape[0] - tokens - up_n

    @pl.when(sp == 0)
    def _():
        kv[0:up_n, :] = jnp.zeros((up_n, 2 * width), BF16)

    @pl.when(sp == ns - 1)
    def _():
        kv[pl.ds(up_n + tokens, down_n), :] = jnp.zeros((down_n, 2 * width), BF16)

    kv[pl.ds(up_n + tokens + down_n, n_keys - down_n), :] = jnp.zeros((n_keys - down_n, 2 * width), BF16)

    def inv_of(x):
        xf = x.astype(F32)
        return lax.rsqrt(jnp.mean(xf * xf, axis=-1, keepdims=True) + EPS)

    ctx_load.wait()
    ctx_inv = inv_of(ctx[...])
    lat_load.wait()
    for t in range(0, tokens, GRID_W):
        inv[t:t + GRID_W, :] = jnp.broadcast_to(inv_of(lat[t:t + GRID_W, :]), (GRID_W, HEAD_DIM))

    wg_load.wait()
    seg = d // 8
    gp = jnp.zeros((8, seg), F32)
    for j in range(8):
        gp = gp + dot(only(row0_act, row == j), wg[:, pl.ds(j * seg, seg)])
    gater[tp] = gp

    def start_gate(o, _):
        tp_copy(gater, gate_s, gate_r, o).start()
        return 0

    lax.fori_loop(1, nt, start_gate, 0)
    wk_load.wait()
    wv_load.wait()

    def wait_mod(o, _):
        tp_copy(modr, mod_s, mod_r, o).wait()
        return 0

    lax.fori_loop(1, nt, wait_mod, 0)
    total = modr[0]
    for i in range(1, nt):
        total = total + modr[i]
    g = gain[...]
    for k in range(2):
        cols = pl.ds(k * half_d, half_d)
        gk = g[:, k * half_d:(k + 1) * half_d]
        mods[0:1, cols] = gk * (1.0 + total[4 * k + 2:4 * k + 3])
        mods[1:2, cols] = total[4 * k:4 * k + 1]
        mods[2:3, cols] = gk * (1.0 + total[4 * k + 3:4 * k + 4])
        mods[3:4, cols] = total[4 * k + 1:4 * k + 2]

    ctx_hid = (ctx[...].astype(F32) * ctx_inv * mods[2:3, :] + mods[3:4, :]).astype(BF16)
    ctx_all[sp % ny, sp // ny] = dot(ctx_hid, wqkv[:, 0:2 * width]).astype(BF16)

    nz = ns // ny
    zi, yi = sp // ny, sp % ny

    def ctx_copy(block, dest, lane):
        return pltpu.make_async_remote_copy(
            src_ref=ctx_all.at[block % ny, block // ny],
            dst_ref=ctx_all.at[block % ny, block // ny],
            send_sem=ctx_s.at[lane, block // ny], recv_sem=ctx_r.at[block],
            device_id={"sp": dest, "tp": tp},
        )

    def across(zb, act):
        def one(o, _):
            act(ctx_copy(zb * ny + yi, zi * ny + (yi + o) % ny, 1 + o))
            return 0

        lax.fori_loop(1, ny, one, 0)

    def upward(zb, act):
        @pl.when(zi < nz - 1)
        def _():
            act(ctx_copy(zb * ny + yi, sp + ny, 0))

    def downward(zb, act):
        @pl.when(zi > 0)
        def _():
            act(ctx_copy(zb * ny + yi, sp - ny, 1))

    def go(c):
        c.start()

    def sent(c):
        c.wait_send()

    def arrived(block):
        ctx_copy(block, sp, 0).wait_recv()

    def relay(k):
        @pl.when(zi - k >= 0)
        def _():
            arrived((zi - k) * ny + yi)
            upward(zi - k, go)
            across(zi - k, go)

        @pl.when(zi + k < nz)
        def _():
            arrived((zi + k) * ny + yi)
            downward(zi + k, go)
            across(zi + k, go)

    upward(zi, go)
    downward(zi, go)
    across(zi, go)

    up = pltpu.make_async_remote_copy(
        src_ref=kv.at[pl.ds(tokens, up_n)], dst_ref=kv.at[pl.ds(0, up_n)],
        send_sem=halo_s.at[0], recv_sem=halo_r.at[0],
        device_id={"sp": (sp + 1) % ns, "tp": tp},
    )
    down = pltpu.make_async_remote_copy(
        src_ref=kv.at[pl.ds(up_n, down_n)], dst_ref=kv.at[pl.ds(up_n + tokens, down_n)],
        send_sem=halo_s.at[1], recv_sem=halo_r.at[1],
        device_id={"sp": (sp + ns - 1) % ns, "tp": tp},
    )
    has_next, has_prev = sp < ns - 1, sp > 0

    wq_load.wait()
    spans = [(tokens - up_n, up_n), (0, down_n), (down_n, tokens - up_n - down_n)]

    def hidden(i):
        lo, n = spans[i]
        x = lat[lo:lo + n, :].astype(F32)
        h = x * wide(inv[lo:lo + n, :], d) * mods[0:1, :] + mods[1:2, :]
        hbuf[i % 2, 0:n, :] = h.astype(BF16)

    hidden(0)
    for i, (lo, n) in enumerate(spans):
        r = dot(hbuf[i % 2, 0:n, :], wqkv[...])
        kv[lo + up_n:lo + up_n + n, :] = r[:, :2 * width].astype(BF16)
        q[lo:lo + n, :] = (r[:, 2 * width:] * q_scale).astype(BF16)
        if i + 1 < len(spans):
            hidden(i + 1)
        if i == 0:
            pl.when(has_next)(lambda: up.start())
        if i == 1:
            pl.when(has_prev)(lambda: down.start())

    half_t = nt // 2
    my_half = tp // half_t
    base_row = sp * rows
    ones = jnp.ones((1, HEAD_DIM), BF16)

    def with_ones(v):
        return jnp.concatenate([v, jnp.broadcast_to(ones, v.shape)], axis=1)

    def window(r):
        grid_row = base_row + r
        s0 = jnp.clip(grid_row - WIN_ROWS // 2, 0, total_rows - WIN_ROWS)
        s1 = jnp.clip(grid_row + 1 - WIN_ROWS // 2, 0, total_rows - WIN_ROWS)
        win = pl.ds(pl.multiple_of((s0 - base_row + UP_ROWS) * GRID_W, GRID_W), KEYS)
        return grid_row, s0, s1, win

    def near_scores(r, h):
        grid_row, s0, s1, win = window(r)
        i0 = s0 - grid_row + WIN_ROWS - 1
        i1 = i0 - 1
        moved = s1 > s0
        lo = h * HEAD_DIM
        t = r * GRID_W
        s = dot_t(q[t:t + PAIR, lo:lo + HEAD_DIM], kv[win, lo:lo + HEAD_DIM])
        b0 = [bias[h, i0 + 2 * k] for k in range(WIN_ROWS // 2)]
        ids = [jnp.where(moved, TABLES, i1)]
        ids += [jnp.where(moved, i1 + 2 * k, i1 + 2 * k) for k in range(1, WIN_ROWS // 2)]
        ids += [jnp.where(moved, TABLES + 1, TABLES + 2)]
        b1 = [bias[h, i] for i in ids]
        x0 = s[:GRID_W, :WIN_ROWS * GRID_W] + jnp.concatenate(b0, axis=1)
        x1 = s[GRID_W:, :] + jnp.concatenate(b1, axis=1)
        s_near[h, t:t + GRID_W, 0:WIN_ROWS * GRID_W] = x0
        s_near[h, t + GRID_W:t + PAIR, :] = x1
        m = jnp.concatenate([jnp.max(x0, axis=-1, keepdims=True), jnp.max(x1, axis=-1, keepdims=True)], axis=0)
        return jnp.broadcast_to(m, (PAIR, HEAD_DIM))

    def near_values(r, h, m):
        win = window(r)[3]
        lo = h * HEAD_DIM
        t = r * GRID_W
        old = mx[h, t:t + PAIR, :]
        m = jnp.maximum(m, old)
        w = jnp.exp2(old - m)
        n0 = WIN_ROWS * GRID_W
        e0 = jnp.exp2(s_near[h, t:t + GRID_W, 0:n0] - wide(m[:GRID_W], n0)).astype(BF16)
        e1 = jnp.exp2(s_near[h, t + GRID_W:t + PAIR, :] - wide(m[GRID_W:], KEYS)).astype(BF16)
        e0 = jnp.concatenate([e0, jnp.zeros((GRID_W, KEYS - n0), BF16)], axis=1)
        p = jnp.concatenate([e0, e1], axis=0)
        o = dot(p, with_ones(kv[win, width + lo:width + lo + HEAD_DIM]))
        mx[h, t:t + PAIR, :] = m
        acc[h, t:t + PAIR, :] = acc[h, t:t + PAIR, :] * wide(w, 2 * HEAD_DIM) + o

    def near(pairs):
        units = [(r, h) for r in pairs for h in range(heads)]
        ms = [near_scores(r, h) for r, h in units]
        for (r, h), m in zip(units, ms):
            near_values(r, h, m)

    def flat(x):
        if c_here % 16:
            return x.astype(F32).reshape(nz * c_here, HEAD_DIM).astype(BF16)
        return x.reshape(nz * c_here, HEAD_DIM)

    far_n = nz * c_here

    def far_scores(t, col, h):
        lo = h * HEAD_DIM
        s = dot_t(q[t, lo:lo + HEAD_DIM], flat(ctx_all[col, :, :, lo:lo + HEAD_DIM]))
        s_far[h, t, :] = s
        return jnp.broadcast_to(jnp.max(s, axis=-1, keepdims=True), (own_n, HEAD_DIM))

    def far_values(t, col, h, m, last):
        lo = h * HEAD_DIM
        old = mx[h, t, :]
        m = jnp.maximum(m, old)
        w = jnp.exp2(old - m)
        e = jnp.exp2(s_far[h, t, :] - wide(m, far_n)).astype(BF16)
        o = dot(e, with_ones(flat(ctx_all[col, :, :, width + lo:width + lo + HEAD_DIM])))
        o = acc[h, t, :] * wide(w, 2 * HEAD_DIM) + o
        if last:
            att[t, lo:lo + HEAD_DIM] = (o[:, :HEAD_DIM] / o[:, HEAD_DIM:]).astype(BF16)
        else:
            mx[h, t, :] = m
            acc[h, t, :] = o

    def far(parts, o, last):
        col = (yi + o) % ny
        units = [(pl.ds(pl.multiple_of(p * own_n, 16), own_n), h) for p in parts for h in range(heads)]
        ms = [far_scores(t, col, h) for t, h in units]
        for (t, h), m in zip(units, ms):
            far_values(t, col, h, m, last)

    def far_all(o, _):
        far(range(nt), o, False)
        return 0

    near(range(UP_ROWS, rows - UP_ROWS, 2))
    relay(1)
    if nz > 2:
        relay(2)
    if nz > 3:
        relay(3)

    def late_relay(k, _):
        relay(k)
        return 0

    lax.fori_loop(4, nz, late_relay, 0)
    if ny > 1:
        far_all(0, 0)

    @pl.when(has_next)
    def _():
        down.wait_recv()
        up.wait_send()

    @pl.when(has_prev)
    def _():
        up.wait_recv()
        down.wait_send()

    near([*range(0, UP_ROWS, 2), *range(rows - UP_ROWS, rows, 2)])

    def settle_row(zb, _):
        def other(o, _):
            arrived(zb * ny + (yi + o) % ny)
            return 0

        lax.fori_loop(1, ny, other, 0)
        across(zb, sent)

        @pl.when(zb <= zi)
        def _():
            upward(zb, sent)

        @pl.when(zb >= zi)
        def _():
            downward(zb, sent)

        return 0

    lax.fori_loop(0, nz, settle_row, 0)

    lax.fori_loop(1, ny - 1, far_all, 0)

    def head_copy(src, dst):
        return pltpu.make_async_remote_copy(
            src_ref=att.at[pl.ds(pl.multiple_of(dst * own_n, 16), own_n)], dst_ref=own.at[src],
            send_sem=head_s.at[dst], recv_sem=head_r.at[src],
            device_id={"sp": sp, "tp": dst},
        )

    other_half = (1 - my_half) * half_t
    far([other_half + j for j in range(half_t)], ny - 1, True)

    def send_other(j, _):
        head_copy(tp, (1 - my_half) * half_t + j).start()
        return 0

    lax.fori_loop(0, half_t, send_other, 0)
    far([my_half * half_t + j for j in range(half_t)], ny - 1, True)

    def mate(o):
        return my_half * half_t + (tp + o) % half_t

    def send_same(o, _):
        head_copy(tp, mate(o)).start()
        return 0

    lax.fori_loop(1, half_t, send_same, 0)

    def wait_gate(o, _):
        tp_copy(gater, gate_s, gate_r, o).wait()
        return 0

    lax.fori_loop(1, nt, wait_gate, 0)
    gsum = gater[0]
    for i in range(1, nt):
        gsum = gsum + gater[i]
    gates[...] = jnp.concatenate([gsum[j:j + 1] for j in range(8)], axis=1)
    own[tp] = att[my_rows, :]
    wo_load.wait()
    own_load.wait()

    def settle(o, _):
        p = (tp + o) % nt
        head_copy(tp, p).wait_send()
        head_copy(p, p).wait_recv()
        return 0

    lax.fori_loop(1, nt, settle, 0)


def finish(own, wo, gates, lat_own, out, buf, sem):
    nt = own.shape[0]
    d = wo.shape[1]
    step = d // 4
    a = jnp.concatenate([own[i] for i in range(nt)], axis=1)
    copies = []
    for i in range(4):
        cols = pl.ds(i * step, step)
        y = dot(a, wo[:, cols])
        buf[:, cols] = (lat_own[:, cols].astype(F32) + gates[:, cols] * y).astype(BF16)
        copies.append(pltpu.make_async_copy(buf.at[:, cols], out.at[:, cols], sem.at[i]))
        copies[-1].start()
    for c in copies:
        c.wait()


def shards(
    ns, nt,
    latents, cond, ctx_cond, context, norm_gain, shift_weight, scale_weight, gate_weight,
    q_weight, k_weight, v_weight, out_weight, rel_bias,
):
    tokens, d = latents.shape
    c_here = context.shape[0]
    kt = shift_weight.shape[0]
    width = q_weight.shape[1]
    heads = width // HEAD_DIM
    own_n = tokens // nt
    table = jnp.transpose(rel_bias, (1, 0, 2))
    ny = 1
    while ns % (2 * ny) == 0 and 4 * ny * ny <= ns:
        ny *= 2
    halo = (UP_ROWS + DOWN_ROWS + 1) * GRID_W
    vmem = pl.BlockSpec(memory_space=pltpu.VMEM)
    hbm = pl.BlockSpec(memory_space=pltpu.HBM)
    sem = pltpu.SemaphoreType.DMA
    tail = 8 * 1024 * 1024
    parts = pl.pallas_call(
        functools.partial(kernel, ns, nt, ny),
        out_shape=(
            pltpu.VMEM((nt, own_n, width), BF16),
            pltpu.VMEM(out_weight.shape, BF16),
            pltpu.VMEM((1, d), F32),
            pltpu.VMEM((own_n, d), BF16),
        ),
        in_specs=[hbm] * 13,
        out_specs=(vmem,) * 4,
        scratch_shapes=[
            pltpu.VMEM((tokens, d), BF16),
            pltpu.VMEM((c_here, d), BF16),
            pltpu.VMEM((kt, d), BF16),
            pltpu.VMEM((kt, d), BF16),
            pltpu.VMEM((kt, d), BF16),
            pltpu.VMEM((d, 3 * width), BF16),
            pltpu.VMEM((nt, 8, d // 2), F32),
            pltpu.VMEM((nt, 8, d // 8), F32),
            pltpu.VMEM((8, d), F32),
            pltpu.VMEM((tokens, HEAD_DIM), F32),
            pltpu.VMEM((2, UP_ROWS * GRID_W, d), BF16),
            pltpu.VMEM((ny, ns // ny, c_here, 2 * width), BF16),
            pltpu.VMEM((tokens + halo, 2 * width), BF16),
            pltpu.VMEM((tokens, width), BF16),
            pltpu.VMEM((heads, TABLES + 3, GRID_W, PAIR), F32),
            pltpu.VMEM((heads, tokens, KEYS), F32),
            pltpu.VMEM((heads, tokens, ns // ny * c_here), F32),
            pltpu.VMEM((heads, tokens, 2 * HEAD_DIM), F32),
            pltpu.VMEM((heads, tokens, HEAD_DIM), F32),
            pltpu.VMEM((tokens, width), BF16),
            pltpu.VMEM((2 * WIN_ROWS - 1, heads, PAIR), F32),
            pltpu.VMEM((1, d), F32),
            pltpu.VMEM((1, d), F32),
            pltpu.VMEM((1, d), F32),
            pltpu.VMEM(table.shape, F32),
            sem((12 + 4 * (d // 2 // 512),)),
            sem((nt,)), sem((nt,)), sem((nt,)), sem((nt,)),
            sem((ny + 1, ns // ny)), sem((ns,)),
            sem((2,)), sem((2,)),
            sem((nt,)), sem((nt,)),
        ],
        compiler_params=pltpu.CompilerParams(
            collective_id=0, has_side_effects=True, vmem_limit_bytes=VMEM_BYTES - tail
        ),
    )(
        cond[None], ctx_cond[None], norm_gain[None], table, latents, context, shift_weight, scale_weight, gate_weight,
        q_weight, k_weight, v_weight, out_weight,
    )
    return pl.pallas_call(
        finish,
        out_shape=jax.ShapeDtypeStruct((own_n, d), BF16),
        in_specs=[vmem] * 4,
        out_specs=hbm,
        scratch_shapes=[pltpu.VMEM((own_n, d), BF16), sem((4,))],
        compiler_params=pltpu.CompilerParams(vmem_limit_bytes=16 * 1024 * 1024),
    )(*parts)


def solution(mesh):
    in_specs = (
        P("sp", None),
        P(),
        P(),
        P("sp", None),
        P(),
        P("tp", None),
        P("tp", None),
        P("tp", None),
        P(None, "tp"),
        P(None, "tp"),
        P(None, "tp"),
        P(),
        P("tp", None, None),
    )
    body = functools.partial(shards, mesh.shape["sp"], mesh.shape["tp"])
    return jax.shard_map(
        body, mesh=mesh, in_specs=in_specs, out_specs=P(("sp", "tp"), None), check_vma=False
    )
```

```python
import functools

import jax
import jax.numpy as jnp
from jax import lax
from jax.experimental import pallas as pl
from jax.experimental.pallas import tpu as pltpu
from jax.sharding import PartitionSpec as P

HEAD_DIM = 128
GRID_W = 64
WIN_ROWS = 8
WIN_COLS = 16
EPS = 1e-06
NEG_BIG = -1e30
F32 = jnp.float32
BF16 = jnp.bfloat16
UP_ROWS = WIN_ROWS // 2
DOWN_ROWS = WIN_ROWS // 2 - 1
PAIR = 2 * GRID_W
KEY_ROWS = WIN_ROWS + 2
KEYS = KEY_ROWS * GRID_W
TABLES = 2 * WIN_ROWS - 2
Z_FIRST = 3
HALO = ((0, 2), (2, 1))
ISSUE = ((), (0,), (1,))
RAW_PARTS = 2
CORES = 2
VMEM_BYTES = 67043328


def dot(a, b):
    return jnp.dot(a, b, preferred_element_type=F32)


def dot_t(a, b):
    return lax.dot_general(a, b, (((1,), (1,)), ((), ())), preferred_element_type=F32)


def wide(x, n):
    return jnp.concatenate([x] * pl.cdiv(n, HEAD_DIM), axis=1)[:, :n]


def kernel(
    ns, nt, ny,
    cond_h, ctx_cond_h, gain_h, table_h,
    lat_h, ctx_h, wsh_h, wsc_h, wg_h, wq_h, wk_h, wv_h, wo_h,
    own, wo, gates, lat_own,
    lat, ctx, wsh, wsc, wg, wqkv,
    modr, gater, mods, inv, hbuf, ctx_all, kv, q, raw, bias, s_near, s_far, acc, mx, att, lines,
    cond, ctx_cond, gain, table,
    load_sem, mod_s, mod_r, gate_s, gate_r, across_s, along_s, ctx_r, halo_s, halo_r, raw_s, raw_r, head_s, head_r,
):
    sp, tp = lax.axis_index("sp"), lax.axis_index("tp")
    tokens, d = lat.shape
    c_here = ctx.shape[0]
    width = q.shape[1]
    heads = width // HEAD_DIM
    kt = wsh.shape[0]
    rows = tokens // GRID_W
    total_rows = rows * ns
    own_n = tokens // nt
    up_n, down_n = UP_ROWS * GRID_W, DOWN_ROWS * GRID_W
    to_log2 = 1.4426950408889634
    q_scale = HEAD_DIM ** -0.5 * to_log2
    half_d = d // 2
    step = 512

    count = [0]

    def load(s, t):
        c = pltpu.make_async_copy(s, t, load_sem.at[count[0]])
        count[0] += 1
        return c

    small = [load(cond_h, cond), load(ctx_cond_h, ctx_cond), load(gain_h, gain), load(table_h, table)]
    mod_loads = []
    for n0 in range(0, half_d, step):
        mod_loads.append([
            load(s.at[:, pl.ds(k * half_d + n0, step)], t.at[:, pl.ds(k * half_d + n0, step)])
            for k in range(2) for s, t in ((wsh_h, wsh), (wsc_h, wsc))
        ])
    ctx_load, lat_load, wg_load = load(ctx_h, ctx), load(lat_h, lat), load(wg_h, wg)
    wk_load = load(wk_h, wqkv.at[:, pl.ds(0, width)])
    wv_load = load(wv_h, wqkv.at[:, pl.ds(width, width)])
    wq_load = load(wq_h, wqkv.at[:, pl.ds(2 * width, width)])
    wo_load = load(wo_h, wo)
    my_rows = pl.ds(pl.multiple_of(tp * own_n, 16), own_n)
    own_load = load(lat_h.at[my_rows], lat_own)
    for c in small + sum(mod_loads, []) + [ctx_load, lat_load]:
        c.start()

    barrier = pltpu.get_barrier_semaphore()

    def greet_tp(o, _):
        pl.semaphore_signal(barrier, inc=1, device_id={"sp": sp, "tp": (tp + o) % nt})
        return 0

    def greet_sp(o, _):
        pl.semaphore_signal(barrier, inc=1, device_id={"sp": (sp + o) % ns, "tp": tp})
        return 0

    lax.fori_loop(1, nt, greet_tp, 0)
    lax.fori_loop(1, ns, greet_sp, 0)

    for c in small:
        c.wait()

    start = pl.multiple_of(tp * kt, 128)
    row = lax.broadcasted_iota(jnp.int32, (8, kt), 0)

    def silu(ref):
        v = ref[:, pl.ds(start, kt)]
        return jnp.broadcast_to(v / (1.0 + jnp.exp(-v)), (8, kt))

    row0_act = silu(cond)
    mixed_act = jnp.where(row % 2 == 0, row0_act, silu(ctx_cond))

    def only(a, keep):
        return jnp.where(keep, a, 0.0).astype(BF16)

    a_sh = [only(mixed_act, (row // 2) == 2 * k) for k in range(2)]
    a_sc = [only(mixed_act, (row // 2) == 2 * k + 1) for k in range(2)]
    def mod_copy(i, o):
        return pltpu.make_async_remote_copy(
            src_ref=modr.at[i, tp], dst_ref=modr.at[i, tp],
            send_sem=mod_s.at[i, o - 1], recv_sem=mod_r.at[i, o - 1],
            device_id={"sp": sp, "tp": (tp + o) % nt},
        )

    def each_mod(i, act):
        def one(o, _):
            act(mod_copy(i, o))
            return 0

        lax.fori_loop(1, nt, one, 0)

    chunks = half_d // step
    for i in range(chunks):
        part = jnp.zeros((8, step), F32)
        for k in range(2):
            cols = pl.ds(k * half_d + i * step, step)
            mod_loads[i][2 * k].wait()
            part = part + dot(a_sh[k], wsh[:, cols])
            mod_loads[i][2 * k + 1].wait()
            part = part + dot(a_sc[k], wsc[:, cols])
        modr[i, tp] = part.astype(BF16)
        if i == 0:
            pl.semaphore_wait(barrier, nt - 1 + ns - 1)
        each_mod(i, lambda c: c.start())
    quarter = up_n // nt
    piece = quarter // RAW_PARTS
    nx = nt // CORES
    core, xi = tp % CORES, tp // CORES
    has_next, has_prev = sp < ns - 1, sp > 0

    def raw_at(i, t):
        return raw.at[pl.ds(pl.multiple_of(t * quarter, 16) + i * piece, piece)]

    def raw_first(i):
        src = lat_h.at[pl.ds(pl.multiple_of(tokens - up_n + tp * quarter, 16) + i * piece, piece)]
        return pltpu.make_async_remote_copy(
            src_ref=src, dst_ref=raw_at(i, tp), send_sem=raw_s.at[i, 0], recv_sem=raw_r.at[i, tp],
            device_id={"sp": (sp + 1) % ns, "tp": tp},
        )

    def raw_next(i, t, dest, lane):
        return pltpu.make_async_remote_copy(
            src_ref=raw_at(i, t), dst_ref=raw_at(i, t), send_sem=raw_s.at[i, lane], recv_sem=raw_r.at[i, t],
            device_id={"sp": sp, "tp": dest},
        )

    def raw_x(i, o):
        return raw_next(i, tp, (xi + o) % nx * CORES + core, o)

    def raw_mate(i, o):
        return raw_next(i, (xi + o) % nx * CORES + core, xi * CORES + (core + 1) % CORES, nx + o)

    def raw_got(i, t):
        raw_next(i, t, tp, 0).wait_recv()

    def raw_along(i):
        @pl.when(has_prev)
        def _():
            raw_got(i, tp)
            for o in range(1, nx):
                raw_x(i, o).start()
            raw_mate(i, 0).start()

    def raw_over(i):
        @pl.when(has_prev)
        def _():
            for o in range(1, nx):
                raw_got(i, (xi + o) % nx * CORES + core)
                raw_mate(i, o).start()

    def raw_done(i):
        @pl.when(has_next)
        def _():
            raw_first(i).wait_send()

        @pl.when(has_prev)
        def _():
            for o in range(nx):
                raw_got(i, (xi + o) % nx * CORES + (core + 1) % CORES)
                raw_mate(i, o).wait_send()
                if o:
                    raw_x(i, o).wait_send()

    @pl.when(has_next)
    def _():
        for i in range(RAW_PARTS):
            raw_first(i).start()

    for c in [wg_load, wk_load, wv_load, wq_load, wo_load, own_load]:
        c.start()

    def tp_copy(buf, s_sem, r_sem, o):
        return pltpu.make_async_remote_copy(
            src_ref=buf.at[tp], dst_ref=buf.at[tp],
            send_sem=s_sem.at[o - 1], recv_sem=r_sem.at[o - 1],
            device_id={"sp": sp, "tp": (tp + o) % nt},
        )

    qc = lax.broadcasted_iota(jnp.int32, (GRID_W, PAIR), 0)
    lane = lax.broadcasted_iota(jnp.int32, (GRID_W, PAIR), 1)
    kc = lane % GRID_W
    first = jnp.clip(qc - WIN_COLS // 2, 0, GRID_W - WIN_COLS)
    inside = (kc >= first) & (kc < first + WIN_COLS)
    lines[...] = jnp.zeros_like(lines)
    lines[:, :, 0:2 * WIN_COLS - 1] = table[...]
    low_row = WIN_ROWS - 1 - WIN_ROWS // 2
    for h in range(heads):
        for i in range(TABLES):
            near_line = jnp.broadcast_to(lines[i, h:h + 1, :], (GRID_W, PAIR))
            next_line = jnp.broadcast_to(lines[i + 1, h:h + 1, :], (GRID_W, PAIR))
            reach = WIN_COLS - 1
            rolled = pltpu.roll(near_line, PAIR - reach, 1, stride=1, stride_axis=0)
            rolled = rolled + pltpu.roll(next_line, GRID_W - reach, 1, stride=1, stride_axis=0)
            both = jnp.where(inside, rolled * to_log2, NEG_BIG)
            bias[h, i] = both
            if i == low_row - 1:
                bias[h, TABLES] = jnp.where(lane >= GRID_W, both, NEG_BIG)
            if i == low_row + WIN_ROWS - 1:
                bias[h, TABLES + 1] = jnp.where(lane < GRID_W, both, NEG_BIG)
        bias[h, TABLES + 2] = jnp.full((GRID_W, PAIR), NEG_BIG, F32)
    mx[...] = jnp.full_like(mx, NEG_BIG)
    acc[...] = jnp.zeros_like(acc)
    n_keys = kv.shape[0] - tokens - up_n

    @pl.when(sp == 0)
    def _():
        raw[...] = jnp.zeros_like(raw)

    @pl.when(sp == ns - 1)
    def _():
        kv[pl.ds(up_n + tokens, down_n), :] = jnp.zeros((down_n, 2 * width), BF16)

    kv[pl.ds(up_n + tokens + down_n, n_keys - down_n), :] = jnp.zeros((n_keys - down_n, 2 * width), BF16)

    def inv_of(x):
        xf = x.astype(F32)
        return lax.rsqrt(jnp.mean(xf * xf, axis=-1, keepdims=True) + EPS)

    ctx_load.wait()
    ctx_inv = inv_of(ctx[...])
    lat_load.wait()
    for t in range(0, tokens, GRID_W):
        inv[t:t + GRID_W, :] = jnp.broadcast_to(inv_of(lat[t:t + GRID_W, :]), (GRID_W, HEAD_DIM))

    wg_load.wait()
    seg = d // 8
    gp = jnp.zeros((8, seg), F32)
    for j in range(8):
        gp = gp + dot(only(row0_act, row == j), wg[:, pl.ds(j * seg, seg)])
    gater[tp] = gp

    def start_gate(o, _):
        tp_copy(gater, gate_s, gate_r, o).start()
        return 0

    lax.fori_loop(1, nt, start_gate, 0)
    wk_load.wait()
    wv_load.wait()

    for i in range(chunks):
        each_mod(i, lambda c: c.wait())
    g = gain[...]
    for i in range(chunks):
        total = modr[i, 0].astype(F32)
        for j in range(1, nt):
            total = total + modr[i, j].astype(F32)
        for k in range(2):
            lo = k * half_d + i * step
            cols = pl.ds(lo, step)
            gk = g[:, lo:lo + step]
            mods[0:1, cols] = gk * (1.0 + total[4 * k + 2:4 * k + 3])
            mods[1:2, cols] = total[4 * k:4 * k + 1]
            mods[2:3, cols] = gk * (1.0 + total[4 * k + 3:4 * k + 4])
            mods[3:4, cols] = total[4 * k + 1:4 * k + 2]

    ctx_hid = (ctx[...].astype(F32) * ctx_inv * mods[2:3, :] + mods[3:4, :]).astype(BF16)
    ctx_all[sp % ny, sp // ny] = dot(ctx_hid, wqkv[:, 0:2 * width]).astype(BF16)

    nz = ns // ny
    zi, yi = sp // ny, sp % ny

    cut = max(Z_FIRST * width // 2 // HEAD_DIM, 1) * HEAD_DIM

    def ctx_copy(part, block, dest, send_sem):
        cols = pl.ds(0, cut) if part == 0 else pl.ds(cut, 2 * width - cut)
        ref = ctx_all.at[block % ny, block // ny, :, cols]
        return pltpu.make_async_remote_copy(
            src_ref=ref, dst_ref=ref, send_sem=send_sem, recv_sem=ctx_r.at[part, block],
            device_id={"sp": dest, "tp": tp},
        )

    def slot(part, block):
        return block + nz if part else block // ny

    def across(part, zb, act):
        def one(o, _):
            act(ctx_copy(part, zb * ny + yi, zi * ny + (yi + o) % ny, across_s.at[part * nz + zb, o - 1]))
            return 0

        lax.fori_loop(1, ny, one, 0)

    def upward(part, block, act):
        @pl.when(zi < nz - 1)
        def _():
            act(ctx_copy(part, block, sp + ny, along_s.at[0, slot(part, block)]))

    def downward(part, block, act):
        @pl.when(zi > 0)
        def _():
            act(ctx_copy(part, block, sp - ny, along_s.at[1, slot(part, block)]))

    def go(c):
        c.start()

    def sent(c):
        c.wait_send()

    def arrived(part, block):
        ctx_copy(part, block, sp, along_s.at[0, slot(part, block)]).wait_recv()

    def beside():
        def one(o, _):
            block = zi * ny + (yi + o) % ny
            arrived(1, block)
            upward(1, block, go)
            downward(1, block, go)
            return 0

        lax.fori_loop(1, ny, one, 0)

    def pass_first(zb, forward):
        block = zb * ny + yi
        arrived(0, block)
        forward(0, block, go)
        across(0, zb, go)

    def pass_second(zb, forward):
        def one(o, _):
            other = zb * ny + (yi + o) % ny
            arrived(1, other)
            forward(1, other, go)
            return 0

        lax.fori_loop(0, ny, one, 0)

    def relay(k, pass_on):
        @pl.when(zi + k < nz)
        def _():
            pass_on(zi + k, downward)

        @pl.when(zi - k >= 0)
        def _():
            pass_on(zi - k, upward)

    across(1, zi, go)
    for part in range(2):
        upward(part, sp, go)
        downward(part, sp, go)
    across(0, zi, go)

    def halo(i):
        lo, n = HALO[i]
        return pltpu.make_async_remote_copy(
            src_ref=kv.at[pl.ds(up_n + lo * GRID_W, n * GRID_W)],
            dst_ref=kv.at[pl.ds(up_n + tokens + lo * GRID_W, n * GRID_W)],
            send_sem=halo_s.at[i], recv_sem=halo_r.at[i],
            device_id={"sp": (sp + ns - 1) % ns, "tp": tp},
        )

    def send_halo(point):
        for i in ISSUE[point]:
            pl.when(has_prev)(lambda c=halo(i): c.start())

    wq_load.wait()
    rest = (tokens - down_n) // 2
    spans = [(0, down_n), (down_n, rest), (down_n + rest, rest)]

    def modulate(x, scale):
        return (x.astype(F32) * scale * mods[0:1, :] + mods[1:2, :]).astype(BF16)

    def hidden(i):
        lo, n = spans[i]
        hbuf[i % 2, 0:n, :] = modulate(lat[lo:lo + n, :], wide(inv[lo:lo + n, :], d))

    hidden(0)
    for i, (lo, n) in enumerate(spans):
        r = dot(hbuf[i % 2, 0:n, :], wqkv[...])
        kv[lo + up_n:lo + up_n + n, :] = r[:, :2 * width].astype(BF16)
        q[lo:lo + n, :] = (r[:, 2 * width:] * q_scale).astype(BF16)
        if i + 1 < len(spans):
            hidden(i + 1)
        if i == 0:
            send_halo(0)
            raw_along(0)
        if i == 1:
            beside()
            send_halo(1)

    half_t = nt // 2
    my_half = tp // half_t
    base_row = sp * rows
    ones = jnp.ones((1, HEAD_DIM), BF16)

    def with_ones(v):
        return jnp.concatenate([v, jnp.broadcast_to(ones, v.shape)], axis=1)

    def window(r):
        grid_row = base_row + r
        s0 = jnp.clip(grid_row - WIN_ROWS // 2, 0, total_rows - WIN_ROWS)
        s1 = jnp.clip(grid_row + 1 - WIN_ROWS // 2, 0, total_rows - WIN_ROWS)
        win = pl.ds(pl.multiple_of((s0 - base_row + UP_ROWS) * GRID_W, GRID_W), KEYS)
        return grid_row, s0, s1, win

    def near_scores(r, h):
        grid_row, s0, s1, win = window(r)
        i0 = s0 - grid_row + WIN_ROWS - 1
        i1 = i0 - 1
        moved = s1 > s0
        lo = h * HEAD_DIM
        t = r * GRID_W
        s = dot_t(q[t:t + PAIR, lo:lo + HEAD_DIM], kv[win, lo:lo + HEAD_DIM])
        b0 = [bias[h, i0 + 2 * k] for k in range(WIN_ROWS // 2)]
        ids = [jnp.where(moved, TABLES, i1)]
        ids += [jnp.where(moved, i1 + 2 * k, i1 + 2 * k) for k in range(1, WIN_ROWS // 2)]
        ids += [jnp.where(moved, TABLES + 1, TABLES + 2)]
        b1 = [bias[h, i] for i in ids]
        x0 = s[:GRID_W, :WIN_ROWS * GRID_W] + jnp.concatenate(b0, axis=1)
        x1 = s[GRID_W:, :] + jnp.concatenate(b1, axis=1)
        s_near[h, t:t + GRID_W, 0:WIN_ROWS * GRID_W] = x0
        s_near[h, t + GRID_W:t + PAIR, :] = x1
        m = jnp.concatenate([jnp.max(x0, axis=-1, keepdims=True), jnp.max(x1, axis=-1, keepdims=True)], axis=0)
        return jnp.broadcast_to(m, (PAIR, HEAD_DIM))

    def near_values(r, h, m):
        win = window(r)[3]
        lo = h * HEAD_DIM
        t = r * GRID_W
        old = mx[h, t:t + PAIR, :]
        m = jnp.maximum(m, old)
        w = jnp.exp2(old - m)
        n0 = WIN_ROWS * GRID_W
        e0 = jnp.exp2(s_near[h, t:t + GRID_W, 0:n0] - wide(m[:GRID_W], n0)).astype(BF16)
        e1 = jnp.exp2(s_near[h, t + GRID_W:t + PAIR, :] - wide(m[GRID_W:], KEYS)).astype(BF16)
        e0 = jnp.concatenate([e0, jnp.zeros((GRID_W, KEYS - n0), BF16)], axis=1)
        p = jnp.concatenate([e0, e1], axis=0)
        o = dot(p, with_ones(kv[win, width + lo:width + lo + HEAD_DIM]))
        mx[h, t:t + PAIR, :] = m
        acc[h, t:t + PAIR, :] = acc[h, t:t + PAIR, :] * wide(w, 2 * HEAD_DIM) + o

    def near(pairs):
        units = [(r, h) for r in pairs for h in range(heads)]
        ms = [near_scores(r, h) for r, h in units]
        for (r, h), m in zip(units, ms):
            near_values(r, h, m)

    def flat(x):
        n = x.shape[0] * c_here
        if c_here % 16:
            return x.astype(F32).reshape(n, HEAD_DIM).astype(BF16)
        return x.reshape(n, HEAD_DIM)

    def far_scores(t, col, zs, h):
        lo = h * HEAD_DIM
        s = dot_t(q[t, lo:lo + HEAD_DIM], flat(ctx_all[col, zs, :, lo:lo + HEAD_DIM]))
        s_far[h, t, 0:s.shape[1]] = s
        return jnp.broadcast_to(jnp.max(s, axis=-1, keepdims=True), (own_n, HEAD_DIM))

    def far_values(t, col, zs, h, m, last):
        lo = width + h * HEAD_DIM
        v = flat(ctx_all[col, zs, :, lo:lo + HEAD_DIM])
        old = mx[h, t, :]
        m = jnp.maximum(m, old)
        w = jnp.exp2(old - m)
        n = v.shape[0]
        e = jnp.exp2(s_far[h, t, 0:n] - wide(m, n)).astype(BF16)
        o = acc[h, t, :] * wide(w, 2 * HEAD_DIM) + dot(e, with_ones(v))
        if last:
            lo = h * HEAD_DIM
            att[t, lo:lo + HEAD_DIM] = (o[:, :HEAD_DIM] / o[:, HEAD_DIM:]).astype(BF16)
        else:
            mx[h, t, :] = m
            acc[h, t, :] = o

    def far(parts, o, zs, last):
        col = (yi + o) % ny
        units = [(pl.ds(pl.multiple_of(p * own_n, 16), own_n), h) for p in parts for h in range(heads)]
        ms = [far_scores(t, col, zs, h) for t, h in units]
        for (t, h), m in zip(units, ms):
            far_values(t, col, zs, h, m, last)

    everything = pl.ds(0, nz)

    def far_all(o, _):
        far(range(nt), o, everything, False)
        return 0

    relay(1, pass_first)
    for i in range(1, RAW_PARTS):
        raw_along(i)
    near(range(UP_ROWS, rows - UP_ROWS, 2))
    relay(1, pass_second)
    send_halo(2)
    raw_over(0)
    if nz > 2:
        relay(2, pass_first)
    if nz > 2:
        relay(2, pass_second)
    for i in range(1, RAW_PARTS):
        raw_over(i)
    for i in range(RAW_PARTS):
        raw_done(i)
    hbuf[0] = modulate(raw[...], inv_of(raw[...]))
    kv[0:up_n, :] = dot(hbuf[0], wqkv[:, 0:2 * width]).astype(BF16)
    near(range(0, UP_ROWS, 2))
    if nz > 3:
        relay(3, pass_first)
    for i in range(len(HALO)):
        pl.when(has_prev)(lambda c=halo(i): c.wait_send())
        pl.when(has_next)(lambda c=halo(i): c.wait_recv())

    near(range(rows - UP_ROWS, rows, 2))

    if nz > 3:
        relay(3, pass_second)

    def late_relay(k, _):
        relay(k, pass_first)
        relay(k, pass_second)
        return 0

    lax.fori_loop(4, nz, late_relay, 0)
    low = zi < nz - nz // 2
    z_last = jnp.where(low, nz - 1, 0)
    z_rest = pl.ds(jnp.where(low, 0, 1), nz - 1)

    def others(zb):
        def other(o, _):
            arrived(0, zb * ny + (yi + o) % ny)
            return 0

        lax.fori_loop(1, ny, other, 0)

    if ny > 1:
        far_all(0, 0)
    for k in range(nz - 1):
        others(z_rest.start + k)
    lax.fori_loop(1, ny - 1, lambda o, c: (far(range(nt), o, z_rest, False), c)[1], 0)
    if nz > 1:
        far(range(nt), ny - 1, z_rest, False)
    others(z_last)
    lax.fori_loop(1, ny - 1, lambda o, c: (far(range(nt), o, pl.ds(z_last, 1), False), c)[1], 0)

    def settle_row(zb, _):
        across(0, zb, sent)

        @pl.when(zb <= zi)
        def _():
            upward(0, zb * ny + yi, sent)

        @pl.when(zb >= zi)
        def _():
            downward(0, zb * ny + yi, sent)

        def column(o, _):
            block = zb * ny + o

            @pl.when(zb <= zi)
            def _():
                upward(1, block, sent)

            @pl.when(zb >= zi)
            def _():
                downward(1, block, sent)

            return 0

        lax.fori_loop(0, ny, column, 0)
        return 0

    def head_copy(src, dst):
        return pltpu.make_async_remote_copy(
            src_ref=att.at[pl.ds(pl.multiple_of(dst * own_n, 16), own_n)], dst_ref=own.at[src],
            send_sem=head_s.at[dst], recv_sem=head_r.at[src],
            device_id={"sp": sp, "tp": dst},
        )

    theirs = [(1 - my_half) * half_t + j for j in range(half_t)]
    ours = [my_half * half_t + (tp + o) % half_t for o in range(half_t)]
    for p in theirs:
        far([p], ny - 1, pl.ds(z_last, 1), True)
        head_copy(tp, p).start()
    far(ours, ny - 1, pl.ds(z_last, 1), True)
    for p in ours[1:]:
        head_copy(tp, p).start()
    across(1, zi, sent)
    lax.fori_loop(0, nz, settle_row, 0)

    def wait_gate(o, _):
        tp_copy(gater, gate_s, gate_r, o).wait()
        return 0

    lax.fori_loop(1, nt, wait_gate, 0)
    gsum = gater[0]
    for i in range(1, nt):
        gsum = gsum + gater[i]
    gates[...] = jnp.concatenate([gsum[j:j + 1] for j in range(8)], axis=1)
    own[tp] = att[my_rows, :]
    wo_load.wait()
    own_load.wait()

    def settle(o, _):
        p = (tp + o) % nt
        head_copy(tp, p).wait_send()
        head_copy(p, p).wait_recv()
        return 0

    lax.fori_loop(1, nt, settle, 0)


def finish(own, wo, gates, lat_own, out, buf, sem):
    nt = own.shape[0]
    d = wo.shape[1]
    step = d // 4
    a = jnp.concatenate([own[i] for i in range(nt)], axis=1)
    copies = []
    for i in range(4):
        cols = pl.ds(i * step, step)
        y = dot(a, wo[:, cols])
        buf[:, cols] = (lat_own[:, cols].astype(F32) + gates[:, cols] * y).astype(BF16)
        copies.append(pltpu.make_async_copy(buf.at[:, cols], out.at[:, cols], sem.at[i]))
        copies[-1].start()
    for c in copies:
        c.wait()


def shards(
    ns, nt,
    latents, cond, ctx_cond, context, norm_gain, shift_weight, scale_weight, gate_weight,
    q_weight, k_weight, v_weight, out_weight, rel_bias,
):
    tokens, d = latents.shape
    c_here = context.shape[0]
    kt = shift_weight.shape[0]
    width = q_weight.shape[1]
    heads = width // HEAD_DIM
    own_n = tokens // nt
    table = jnp.transpose(rel_bias, (1, 0, 2))
    ny = 1
    while ns % (2 * ny) == 0 and 4 * ny * ny <= ns:
        ny *= 2
    halo = (UP_ROWS + DOWN_ROWS + 1) * GRID_W
    vmem = pl.BlockSpec(memory_space=pltpu.VMEM)
    hbm = pl.BlockSpec(memory_space=pltpu.HBM)
    sem = pltpu.SemaphoreType.DMA
    tail = 8 * 1024 * 1024
    parts = pl.pallas_call(
        functools.partial(kernel, ns, nt, ny),
        out_shape=(
            pltpu.VMEM((nt, own_n, width), BF16),
            pltpu.VMEM(out_weight.shape, BF16),
            pltpu.VMEM((1, d), F32),
            pltpu.VMEM((own_n, d), BF16),
        ),
        in_specs=[hbm] * 13,
        out_specs=(vmem,) * 4,
        scratch_shapes=[
            pltpu.VMEM((tokens, d), BF16),
            pltpu.VMEM((c_here, d), BF16),
            pltpu.VMEM((kt, d), BF16),
            pltpu.VMEM((kt, d), BF16),
            pltpu.VMEM((kt, d), BF16),
            pltpu.VMEM((d, 3 * width), BF16),
            pltpu.VMEM((d // 2 // 512, nt, 8, 512), BF16),
            pltpu.VMEM((nt, 8, d // 8), F32),
            pltpu.VMEM((8, d), F32),
            pltpu.VMEM((tokens, HEAD_DIM), F32),
            pltpu.VMEM((2, UP_ROWS * GRID_W, d), BF16),
            pltpu.VMEM((ny, ns // ny, c_here, 2 * width), BF16),
            pltpu.VMEM((tokens + halo, 2 * width), BF16),
            pltpu.VMEM((tokens, width), BF16),
            pltpu.VMEM((UP_ROWS * GRID_W, d), BF16),
            pltpu.VMEM((heads, TABLES + 3, GRID_W, PAIR), F32),
            pltpu.VMEM((heads, tokens, KEYS), F32),
            pltpu.VMEM((heads, tokens, ns // ny * c_here), F32),
            pltpu.VMEM((heads, tokens, 2 * HEAD_DIM), F32),
            pltpu.VMEM((heads, tokens, HEAD_DIM), F32),
            pltpu.VMEM((tokens, width), BF16),
            pltpu.VMEM((2 * WIN_ROWS - 1, heads, PAIR), F32),
            pltpu.VMEM((1, d), F32),
            pltpu.VMEM((1, d), F32),
            pltpu.VMEM((1, d), F32),
            pltpu.VMEM(table.shape, F32),
            sem((12 + 4 * (d // 2 // 512),)),
            sem((d // 2 // 512, nt - 1)), sem((d // 2 // 512, nt - 1)), sem((nt - 1,)), sem((nt - 1,)),
            sem((2 * (ns // ny), max(ny - 1, 1))), sem((2, ns + ns // ny)), sem((2, ns)),
            sem((len(HALO),)), sem((len(HALO),)),
            sem((RAW_PARTS, 2 * (nt // CORES))), sem((RAW_PARTS, nt)),
            sem((nt,)), sem((nt,)),
        ],
        compiler_params=pltpu.CompilerParams(
            collective_id=0, has_side_effects=True, vmem_limit_bytes=VMEM_BYTES - tail
        ),
    )(
        cond[None], ctx_cond[None], norm_gain[None], table, latents, context, shift_weight, scale_weight, gate_weight,
        q_weight, k_weight, v_weight, out_weight,
    )
    return pl.pallas_call(
        finish,
        out_shape=jax.ShapeDtypeStruct((own_n, d), BF16),
        in_specs=[vmem] * 4,
        out_specs=hbm,
        scratch_shapes=[pltpu.VMEM((own_n, d), BF16), sem((4,))],
        compiler_params=pltpu.CompilerParams(vmem_limit_bytes=16 * 1024 * 1024),
    )(*parts)


def solution(mesh):
    in_specs = (
        P("sp", None),
        P(),
        P(),
        P("sp", None),
        P(),
        P("tp", None),
        P("tp", None),
        P("tp", None),
        P(None, "tp"),
        P(None, "tp"),
        P(None, "tp"),
        P(),
        P("tp", None, None),
    )
    body = functools.partial(shards, mesh.shape["sp"], mesh.shape["tp"])
    return jax.shard_map(
        body, mesh=mesh, in_specs=in_specs, out_specs=P(("sp", "tp"), None), check_vma=False
    )
```

```python
import functools

import jax
import jax.numpy as jnp
from jax import lax
from jax.experimental import pallas as pl
from jax.experimental.pallas import tpu as pltpu
from jax.sharding import PartitionSpec as P

HEAD_DIM = 128
GRID_W = 64
WIN_ROWS = 8
WIN_COLS = 16
EPS = 1e-06
NEG_BIG = -1e30
F32 = jnp.float32
BF16 = jnp.bfloat16
UP_ROWS = WIN_ROWS // 2
DOWN_ROWS = WIN_ROWS // 2 - 1
PAIR = 2 * GRID_W
KEY_ROWS = WIN_ROWS + 2
KEYS = KEY_ROWS * GRID_W
TABLES = 2 * WIN_ROWS - 2
Z_FIRST = 3
HALO = ((0, 2), (2, 2))
ISSUE = ((), (0,), (), (1,))
RAW_PARTS = 1
CORES = 2
VMEM_BYTES = 67043328


def dot(a, b):
    return jnp.dot(a, b, preferred_element_type=F32)


def dot_t(a, b):
    return lax.dot_general(a, b, (((1,), (1,)), ((), ())), preferred_element_type=F32)


def wide(x, n):
    return jnp.concatenate([x] * pl.cdiv(n, HEAD_DIM), axis=1)[:, :n]


def kernel(
    ns, nt, ny,
    cond_h, ctx_cond_h, gain_h, table_h,
    lat_h, ctx_h, wsh_h, wsc_h, wg_h, wq_h, wk_h, wv_h, wo_h,
    own, wo, gates, lat_own,
    lat, ctx, wsh, wsc, wg, wqkv,
    modr, gater, mods, inv, hbuf, ctx_all, kv, q, raw, bias, s_near, s_far, acc, mx, att, lines,
    cond, ctx_cond, gain, table,
    load_sem, mod_s, mod_r, gate_s, gate_r, across_s, along_s, ctx_r, halo_s, halo_r, raw_s, raw_r, head_s, head_r,
):
    sp, tp = lax.axis_index("sp"), lax.axis_index("tp")
    tokens, d = lat.shape
    c_here = ctx.shape[0]
    width = q.shape[1]
    heads = width // HEAD_DIM
    kt = wsh.shape[0]
    rows = tokens // GRID_W
    total_rows = rows * ns
    own_n = tokens // nt
    up_n, down_n = UP_ROWS * GRID_W, DOWN_ROWS * GRID_W
    to_log2 = 1.4426950408889634
    q_scale = HEAD_DIM ** -0.5 * to_log2
    half_d = d // 2
    step = 512

    count = [0]

    def load(s, t, same=None):
        if same is None:
            same = count[0]
            count[0] += 1
        return pltpu.make_async_copy(s, t, load_sem.at[same])

    small = [load(cond_h, cond), load(ctx_cond_h, ctx_cond), load(gain_h, gain), load(table_h, table)]
    mod_loads, mod_slots = [], []
    for n0 in range(0, half_d, step):
        slot_here = count[0]
        mod_slots.append(slot_here)
        count[0] += 1
        mod_loads.append([
            load(s.at[:, pl.ds(k * half_d + n0, step)], t.at[:, pl.ds(k * half_d + n0, step)], slot_here)
            for k in range(2) for s, t in ((wsh_h, wsh), (wsc_h, wsc))
        ])
    ctx_load, lat_load, wg_load = load(ctx_h, ctx), load(lat_h, lat), load(wg_h, wg)
    wk_load = load(wk_h, wqkv.at[:, pl.ds(0, width)])
    wv_load = load(wv_h, wqkv.at[:, pl.ds(width, width)])
    wq_load = load(wq_h, wqkv.at[:, pl.ds(2 * width, width)])
    wo_load = load(wo_h, wo)
    my_rows = pl.ds(pl.multiple_of(tp * own_n, 16), own_n)
    own_load = load(lat_h.at[my_rows], lat_own)
    for c in small + sum(mod_loads, []) + [ctx_load, lat_load]:
        c.start()

    barrier = pltpu.get_barrier_semaphore()

    def greet_tp(o, _):
        pl.semaphore_signal(barrier, inc=1, device_id={"sp": sp, "tp": (tp + o) % nt})
        return 0

    def greet_sp(o, _):
        pl.semaphore_signal(barrier, inc=1, device_id={"sp": (sp + o) % ns, "tp": tp})
        return 0

    lax.fori_loop(1, nt, greet_tp, 0)
    lax.fori_loop(1, ns, greet_sp, 0)

    for c in small:
        c.wait()

    start = pl.multiple_of(tp * kt, 128)
    row = lax.broadcasted_iota(jnp.int32, (8, kt), 0)

    def silu(ref):
        v = ref[:, pl.ds(start, kt)]
        return jnp.broadcast_to(v / (1.0 + jnp.exp(-v)), (8, kt))

    row0_act = silu(cond)
    mixed_act = jnp.where(row % 2 == 0, row0_act, silu(ctx_cond))

    def only(a, keep):
        return jnp.where(keep, a, 0.0).astype(BF16)

    a_sh = [only(mixed_act, (row // 2) == 2 * k) for k in range(2)]
    a_sc = [only(mixed_act, (row // 2) == 2 * k + 1) for k in range(2)]
    def mod_copy(i, o):
        return pltpu.make_async_remote_copy(
            src_ref=modr.at[i, tp], dst_ref=modr.at[i, tp],
            send_sem=mod_s.at[o - 1], recv_sem=mod_r.at[o - 1],
            device_id={"sp": sp, "tp": (tp + o) % nt},
        )

    def each_mod(i, act):
        def one(o, _):
            act(mod_copy(i, o))
            return 0

        lax.fori_loop(1, nt, one, 0)

    chunks = half_d // step
    for i in range(chunks):
        load(wsh_h.at[:, pl.ds(0, 4 * step)], wsh.at[:, pl.ds(0, 4 * step)], mod_slots[i]).wait()
        part = jnp.zeros((8, step), F32)
        for k in range(2):
            cols = pl.ds(k * half_d + i * step, step)
            part = part + dot(a_sh[k], wsh[:, cols])
            part = part + dot(a_sc[k], wsc[:, cols])
        modr[i, tp] = part
        if i == 0:
            pl.semaphore_wait(barrier, nt - 1 + ns - 1)
        each_mod(i, lambda c: c.start())
    quarter = down_n // nt
    piece = quarter // RAW_PARTS
    nx = nt // CORES
    core, xi = tp % CORES, tp // CORES
    has_next, has_prev = sp < ns - 1, sp > 0

    def raw_at(i, t):
        return raw.at[pl.ds(pl.multiple_of(t * quarter, 8) + i * piece, piece)]

    def raw_first(i):
        src = lat_h.at[pl.ds(pl.multiple_of(tp * quarter, 8) + i * piece, piece)]
        return pltpu.make_async_remote_copy(
            src_ref=src, dst_ref=raw_at(i, tp), send_sem=raw_s.at[i, 0], recv_sem=raw_r.at[i, tp],
            device_id={"sp": (sp + ns - 1) % ns, "tp": tp},
        )

    def raw_next(i, t, dest, lane):
        return pltpu.make_async_remote_copy(
            src_ref=raw_at(i, t), dst_ref=raw_at(i, t), send_sem=raw_s.at[i, lane], recv_sem=raw_r.at[i, t],
            device_id={"sp": sp, "tp": dest},
        )

    def raw_x(i, o):
        return raw_next(i, tp, (xi + o) % nx * CORES + core, o)

    def raw_mate(i, o):
        return raw_next(i, (xi + o) % nx * CORES + core, xi * CORES + (core + 1) % CORES, nx + o)

    def raw_got(i, t):
        raw_next(i, t, tp, 0).wait_recv()

    def raw_along(i):
        @pl.when(has_next)
        def _():
            raw_got(i, tp)
            for o in range(1, nx):
                raw_x(i, o).start()
            raw_mate(i, 0).start()

    def raw_over(i):
        @pl.when(has_next)
        def _():
            for o in range(1, nx):
                raw_got(i, (xi + o) % nx * CORES + core)
                raw_mate(i, o).start()

    def raw_done(i):
        @pl.when(has_prev)
        def _():
            raw_first(i).wait_send()

        @pl.when(has_next)
        def _():
            for o in range(nx):
                raw_got(i, (xi + o) % nx * CORES + (core + 1) % CORES)
                raw_mate(i, o).wait_send()
                if o:
                    raw_x(i, o).wait_send()

    @pl.when(has_prev)
    def _():
        for i in range(RAW_PARTS):
            raw_first(i).start()

    for c in [wg_load, wk_load, wv_load, wq_load, wo_load, own_load]:
        c.start()

    def tp_copy(buf, s_sem, r_sem, o):
        return pltpu.make_async_remote_copy(
            src_ref=buf.at[tp], dst_ref=buf.at[tp],
            send_sem=s_sem.at[o - 1], recv_sem=r_sem.at[o - 1],
            device_id={"sp": sp, "tp": (tp + o) % nt},
        )

    qc = lax.broadcasted_iota(jnp.int32, (GRID_W, PAIR), 0)
    lane = lax.broadcasted_iota(jnp.int32, (GRID_W, PAIR), 1)
    kc = lane % GRID_W
    first = jnp.clip(qc - WIN_COLS // 2, 0, GRID_W - WIN_COLS)
    inside = (kc >= first) & (kc < first + WIN_COLS)
    lines[...] = jnp.zeros_like(lines)
    lines[:, :, 0:2 * WIN_COLS - 1] = table[...]
    low_row = WIN_ROWS - 1 - WIN_ROWS // 2
    for h in range(heads):
        for i in range(TABLES):
            near_line = jnp.broadcast_to(lines[i, h:h + 1, :], (GRID_W, PAIR))
            next_line = jnp.broadcast_to(lines[i + 1, h:h + 1, :], (GRID_W, PAIR))
            reach = WIN_COLS - 1
            rolled = pltpu.roll(near_line, PAIR - reach, 1, stride=1, stride_axis=0)
            rolled = rolled + pltpu.roll(next_line, GRID_W - reach, 1, stride=1, stride_axis=0)
            both = jnp.where(inside, rolled * to_log2, NEG_BIG)
            bias[h, i] = both
            if i == low_row - 1:
                bias[h, TABLES] = jnp.where(lane >= GRID_W, both, NEG_BIG)
            if i == low_row + WIN_ROWS - 1:
                bias[h, TABLES + 1] = jnp.where(lane < GRID_W, both, NEG_BIG)
        bias[h, TABLES + 2] = jnp.full((GRID_W, PAIR), NEG_BIG, F32)
    mx[...] = jnp.full_like(mx, NEG_BIG)
    acc[...] = jnp.zeros_like(acc)
    n_keys = kv.shape[0] - tokens - up_n

    @pl.when(sp == ns - 1)
    def _():
        raw[...] = jnp.zeros_like(raw)

    @pl.when(sp == 0)
    def _():
        kv[0:up_n, :] = jnp.zeros((up_n, 2 * width), BF16)

    kv[pl.ds(up_n + tokens + down_n, n_keys - down_n), :] = jnp.zeros((n_keys - down_n, 2 * width), BF16)

    def inv_of(x):
        xf = x.astype(F32)
        return lax.rsqrt(jnp.mean(xf * xf, axis=-1, keepdims=True) + EPS)

    ctx_load.wait()
    ctx_inv = inv_of(ctx[...])
    lat_load.wait()
    for t in range(0, tokens, GRID_W):
        inv[t:t + GRID_W, :] = jnp.broadcast_to(inv_of(lat[t:t + GRID_W, :]), (GRID_W, HEAD_DIM))

    wg_load.wait()
    seg = d // 8
    gp = jnp.zeros((8, seg), F32)
    for j in range(8):
        gp = gp + dot(only(row0_act, row == j), wg[:, pl.ds(j * seg, seg)])
    gater[tp] = gp

    def start_gate(o, _):
        tp_copy(gater, gate_s, gate_r, o).start()
        return 0

    lax.fori_loop(1, nt, start_gate, 0)
    wk_load.wait()
    wv_load.wait()

    each_mod(pl.ds(0, chunks), lambda c: c.wait())
    g = gain[...]
    for i in range(chunks):
        total = modr[i, 0]
        for j in range(1, nt):
            total = total + modr[i, j]
        for k in range(2):
            lo = k * half_d + i * step
            cols = pl.ds(lo, step)
            gk = g[:, lo:lo + step]
            mods[0:1, cols] = gk * (1.0 + total[4 * k + 2:4 * k + 3])
            mods[1:2, cols] = total[4 * k:4 * k + 1]
            mods[2:3, cols] = gk * (1.0 + total[4 * k + 3:4 * k + 4])
            mods[3:4, cols] = total[4 * k + 1:4 * k + 2]

    ctx_hid = (ctx[...].astype(F32) * ctx_inv * mods[2:3, :] + mods[3:4, :]).astype(BF16)
    ctx_all[sp % ny, sp // ny] = dot(ctx_hid, wqkv[:, 0:2 * width]).astype(BF16)

    nz = ns // ny
    zi, yi = sp // ny, sp % ny

    cut = max(Z_FIRST * width // 2 // HEAD_DIM, 1) * HEAD_DIM

    def ctx_copy(part, block, dest, send_sem):
        cols = (pl.ds(0, cut), pl.ds(cut, 2 * width - cut), pl.ds(0, 2 * width))[part]
        ref = ctx_all.at[block % ny, block // ny, :, cols]
        return pltpu.make_async_remote_copy(
            src_ref=ref, dst_ref=ref, send_sem=send_sem, recv_sem=ctx_r.at[part % 2, block],
            device_id={"sp": dest, "tp": tp},
        )

    def across(part, zb, act):
        def one(o, _):
            act(ctx_copy(part, zb * ny + yi, zi * ny + (yi + o) % ny, across_s.at[zb, o - 1]))
            return 0

        lax.fori_loop(1, ny, one, 0)

    def upward(part, block, act):
        @pl.when(zi < nz - 1)
        def _():
            act(ctx_copy(part, block, sp + ny, along_s.at[0, block]))

    def downward(part, block, act):
        @pl.when(zi > 0)
        def _():
            act(ctx_copy(part, block, sp - ny, along_s.at[1, block]))

    def go(c):
        c.start()

    def sent(c):
        c.wait_send()

    def arrived(part, block):
        ctx_copy(part, block, sp, along_s.at[0, block]).wait_recv()

    def beside():
        def one(o, _):
            block = zi * ny + (yi + o) % ny
            arrived(1, block)
            upward(1, block, go)
            downward(1, block, go)
            return 0

        lax.fori_loop(1, ny, one, 0)

    def pass_first(zb, forward):
        block = zb * ny + yi
        arrived(0, block)
        forward(0, block, go)
        across(0, zb, go)

    def pass_second(zb, forward):
        def one(o, _):
            other = zb * ny + (yi + o) % ny
            arrived(1, other)
            forward(1, other, go)
            return 0

        lax.fori_loop(0, ny, one, 0)

    def relay(k, pass_on):
        @pl.when(zi + k < nz)
        def _():
            pass_on(zi + k, downward)

        @pl.when(zi - k >= 0)
        def _():
            pass_on(zi - k, upward)

    across(1, zi, go)
    for part in range(2):
        upward(part, sp, go)
        downward(part, sp, go)
    across(0, zi, go)

    def halo(i):
        lo, n = HALO[i]
        return pltpu.make_async_remote_copy(
            src_ref=kv.at[pl.ds(tokens + lo * GRID_W, n * GRID_W)],
            dst_ref=kv.at[pl.ds(lo * GRID_W, n * GRID_W)],
            send_sem=halo_s.at[i], recv_sem=halo_r.at[i],
            device_id={"sp": (sp + 1) % ns, "tp": tp},
        )

    def send_halo(point):
        for i in ISSUE[point]:
            pl.when(has_next)(lambda c=halo(i): c.start())

    wq_load.wait()
    rest = (tokens - up_n) // 2
    spans = [(tokens - up_n, up_n), (0, rest), (rest, rest)]

    def modulate(x, scale):
        return (x.astype(F32) * scale * mods[0:1, :] + mods[1:2, :]).astype(BF16)

    def hidden(i):
        lo, n = spans[i]
        hbuf[i % 2, 0:n, :] = modulate(lat[lo:lo + n, :], wide(inv[lo:lo + n, :], d))

    hidden(0)
    for i, (lo, n) in enumerate(spans):
        r = dot(hbuf[i % 2, 0:n, :], wqkv[...])
        kv[lo + up_n:lo + up_n + n, :] = r[:, :2 * width].astype(BF16)
        q[lo:lo + n, :] = (r[:, 2 * width:] * q_scale).astype(BF16)
        if i + 1 < len(spans):
            hidden(i + 1)
        if i == 0:
            send_halo(0)
            raw_along(0)
        if i == 1:
            beside()
            send_halo(1)

    half_t = nt // 2
    my_half = tp // half_t
    base_row = sp * rows
    ones = jnp.ones((1, HEAD_DIM), BF16)

    def with_ones(v):
        return jnp.concatenate([v, jnp.broadcast_to(ones, v.shape)], axis=1)

    def window(r):
        grid_row = base_row + r
        s0 = jnp.clip(grid_row - WIN_ROWS // 2, 0, total_rows - WIN_ROWS)
        s1 = jnp.clip(grid_row + 1 - WIN_ROWS // 2, 0, total_rows - WIN_ROWS)
        win = pl.ds(pl.multiple_of((s0 - base_row + UP_ROWS) * GRID_W, GRID_W), KEYS)
        return grid_row, s0, s1, win

    def near_scores(r, h):
        grid_row, s0, s1, win = window(r)
        i0 = s0 - grid_row + WIN_ROWS - 1
        i1 = i0 - 1
        moved = s1 > s0
        lo = h * HEAD_DIM
        t = r * GRID_W
        s = dot_t(q[t:t + PAIR, lo:lo + HEAD_DIM], kv[win, lo:lo + HEAD_DIM])
        b0 = [bias[h, i0 + 2 * k] for k in range(WIN_ROWS // 2)]
        ids = [jnp.where(moved, TABLES, i1)]
        ids += [jnp.where(moved, i1 + 2 * k, i1 + 2 * k) for k in range(1, WIN_ROWS // 2)]
        ids += [jnp.where(moved, TABLES + 1, TABLES + 2)]
        b1 = [bias[h, i] for i in ids]
        x0 = s[:GRID_W, :WIN_ROWS * GRID_W] + jnp.concatenate(b0, axis=1)
        x1 = s[GRID_W:, :] + jnp.concatenate(b1, axis=1)
        s_near[h, t:t + GRID_W, 0:WIN_ROWS * GRID_W] = x0
        s_near[h, t + GRID_W:t + PAIR, :] = x1
        m = jnp.concatenate([jnp.max(x0, axis=-1, keepdims=True), jnp.max(x1, axis=-1, keepdims=True)], axis=0)
        return jnp.broadcast_to(m, (PAIR, HEAD_DIM))

    def near_values(r, h, m):
        win = window(r)[3]
        lo = h * HEAD_DIM
        t = r * GRID_W
        old = mx[h, t:t + PAIR, :]
        m = jnp.maximum(m, old)
        w = jnp.exp2(old - m)
        n0 = WIN_ROWS * GRID_W
        e0 = jnp.exp2(s_near[h, t:t + GRID_W, 0:n0] - wide(m[:GRID_W], n0)).astype(BF16)
        e1 = jnp.exp2(s_near[h, t + GRID_W:t + PAIR, :] - wide(m[GRID_W:], KEYS)).astype(BF16)
        e0 = jnp.concatenate([e0, jnp.zeros((GRID_W, KEYS - n0), BF16)], axis=1)
        p = jnp.concatenate([e0, e1], axis=0)
        o = dot(p, with_ones(kv[win, width + lo:width + lo + HEAD_DIM]))
        mx[h, t:t + PAIR, :] = m
        acc[h, t:t + PAIR, :] = acc[h, t:t + PAIR, :] * wide(w, 2 * HEAD_DIM) + o

    def near(pairs):
        units = [(r, h) for r in pairs for h in range(heads)]
        ms = [near_scores(r, h) for r, h in units]
        for (r, h), m in zip(units, ms):
            near_values(r, h, m)

    def flat(x):
        n = x.shape[0] * c_here
        if c_here % 16:
            return x.astype(F32).reshape(n, HEAD_DIM).astype(BF16)
        return x.reshape(n, HEAD_DIM)

    def far_scores(t, col, zs, h):
        lo = h * HEAD_DIM
        s = dot_t(q[t, lo:lo + HEAD_DIM], flat(ctx_all[col, zs, :, lo:lo + HEAD_DIM]))
        s_far[h, t, 0:s.shape[1]] = s
        return jnp.broadcast_to(jnp.max(s, axis=-1, keepdims=True), (own_n, HEAD_DIM))

    def far_values(t, col, zs, h, m, last):
        lo = width + h * HEAD_DIM
        v = flat(ctx_all[col, zs, :, lo:lo + HEAD_DIM])
        old = mx[h, t, :]
        m = jnp.maximum(m, old)
        w = jnp.exp2(old - m)
        n = v.shape[0]
        e = jnp.exp2(s_far[h, t, 0:n] - wide(m, n)).astype(BF16)
        o = acc[h, t, :] * wide(w, 2 * HEAD_DIM) + dot(e, with_ones(v))
        if last:
            lo = h * HEAD_DIM
            att[t, lo:lo + HEAD_DIM] = (o[:, :HEAD_DIM] / o[:, HEAD_DIM:]).astype(BF16)
        else:
            mx[h, t, :] = m
            acc[h, t, :] = o

    def far(parts, o, zs, last):
        col = (yi + o) % ny
        units = [(pl.ds(pl.multiple_of(p * own_n, 16), own_n), h) for p in parts for h in range(heads)]
        ms = [far_scores(t, col, zs, h) for t, h in units]
        for (t, h), m in zip(units, ms):
            far_values(t, col, zs, h, m, last)

    everything = pl.ds(0, nz)

    def far_all(o, _):
        far(range(nt), o, everything, False)
        return 0

    relay(1, pass_first)
    for i in range(1, RAW_PARTS):
        raw_along(i)
    near(range(UP_ROWS, rows - UP_ROWS, 2))
    relay(1, pass_second)
    send_halo(2)
    if nz > 2:
        relay(2, pass_first)
    send_halo(3)
    for i in range(RAW_PARTS):
        raw_over(i)
    if nz > 2:
        relay(2, pass_second)
    for i in range(RAW_PARTS):
        raw_done(i)
    hbuf[0, 0:down_n, :] = modulate(raw[...], inv_of(raw[...]))
    below = dot(hbuf[0, 0:down_n, :], wqkv[:, 0:2 * width])
    kv[up_n + tokens:up_n + tokens + down_n, :] = below.astype(BF16)
    near(range(rows - UP_ROWS, rows, 2))
    if nz > 3:
        relay(3, pass_first)
    if nz > 3:
        relay(3, pass_second)

    def late_relay(k, _):
        relay(k, pass_first)
        relay(k, pass_second)
        return 0

    lax.fori_loop(4, nz, late_relay, 0)
    low = zi < nz - nz // 2
    z_last = jnp.where(low, nz - 1, 0)
    z_rest = pl.ds(jnp.where(low, 0, 1), nz - 1)

    def others(zb):
        def other(o, _):
            arrived(0, zb * ny + (yi + o) % ny)
            return 0

        lax.fori_loop(1, ny, other, 0)

    if ny > 1:
        far_all(0, 0)
    for k in range(nz - 1):
        others(z_rest.start + k)
    lax.fori_loop(1, ny - 1, lambda o, c: (far(range(nt), o, z_rest, False), c)[1], 0)
    if nz > 1:
        far(range(nt), ny - 1, z_rest, False)
    for i in range(len(HALO)):
        pl.when(has_next)(lambda c=halo(i): c.wait_send())
        pl.when(has_prev)(lambda c=halo(i): c.wait_recv())

    near(range(0, UP_ROWS, 2))

    others(z_last)
    lax.fori_loop(1, ny - 1, lambda o, c: (far(range(nt), o, pl.ds(z_last, 1), False), c)[1], 0)

    def settle_row(zb, _):
        pl.when(zb == zi)(lambda: across(2, zb, sent))
        pl.when(zb != zi)(lambda: across(0, zb, sent))

        @pl.when(zb <= zi)
        def _():
            upward(2, zb * ny + yi, sent)

        @pl.when(zb >= zi)
        def _():
            downward(2, zb * ny + yi, sent)

        def column(o, _):
            block = zb * ny + (yi + o) % ny

            @pl.when(zb <= zi)
            def _():
                upward(1, block, sent)

            @pl.when(zb >= zi)
            def _():
                downward(1, block, sent)

            return 0

        lax.fori_loop(1, ny, column, 0)
        return 0

    def head_copy(src, dst):
        return pltpu.make_async_remote_copy(
            src_ref=att.at[pl.ds(pl.multiple_of(dst * own_n, 16), own_n)], dst_ref=own.at[src],
            send_sem=head_s.at[(dst - src + nt - 1) % nt], recv_sem=head_r.at[(dst - src + nt - 1) % nt],
            device_id={"sp": sp, "tp": dst},
        )

    theirs = [(1 - my_half) * half_t + j for j in range(half_t)]
    ours = [my_half * half_t + (tp + o) % half_t for o in range(half_t)]
    for p in theirs:
        far([p], ny - 1, pl.ds(z_last, 1), True)
        head_copy(tp, p).start()
    far(ours, ny - 1, pl.ds(z_last, 1), True)
    for p in ours[1:]:
        head_copy(tp, p).start()
    lax.fori_loop(0, nz, settle_row, 0)

    def wait_gate(o, _):
        tp_copy(gater, gate_s, gate_r, o).wait()
        return 0

    lax.fori_loop(1, nt, wait_gate, 0)
    gsum = gater[0]
    for i in range(1, nt):
        gsum = gsum + gater[i]
    gates[...] = jnp.concatenate([gsum[j:j + 1] for j in range(8)], axis=1)
    own[tp] = att[my_rows, :]
    wo_load.wait()
    own_load.wait()

    def settle(o, _):
        p = (tp + o) % nt
        head_copy(tp, p).wait_send()
        head_copy(p, tp).wait_recv()
        return 0

    lax.fori_loop(1, nt, settle, 0)


def finish(own, wo, gates, lat_own, out, buf, sem):
    nt = own.shape[0]
    d = wo.shape[1]
    step = d // 4
    a = jnp.concatenate([own[i] for i in range(nt)], axis=1)
    copies = []
    for i in range(4):
        cols = pl.ds(i * step, step)
        y = dot(a, wo[:, cols])
        buf[:, cols] = (lat_own[:, cols].astype(F32) + gates[:, cols] * y).astype(BF16)
        copies.append(pltpu.make_async_copy(buf.at[:, cols], out.at[:, cols], sem.at[i]))
        copies[-1].start()
    for c in copies:
        c.wait()


def shards(
    ns, nt,
    latents, cond, ctx_cond, context, norm_gain, shift_weight, scale_weight, gate_weight,
    q_weight, k_weight, v_weight, out_weight, rel_bias,
):
    tokens, d = latents.shape
    c_here = context.shape[0]
    kt = shift_weight.shape[0]
    width = q_weight.shape[1]
    heads = width // HEAD_DIM
    own_n = tokens // nt
    table = jnp.transpose(rel_bias, (1, 0, 2))
    ny = 1
    while ns % (2 * ny) == 0 and 4 * ny * ny <= ns:
        ny *= 2
    halo = (UP_ROWS + DOWN_ROWS + 1) * GRID_W
    vmem = pl.BlockSpec(memory_space=pltpu.VMEM)
    hbm = pl.BlockSpec(memory_space=pltpu.HBM)
    sem = pltpu.SemaphoreType.DMA
    tail = 8 * 1024 * 1024
    parts = pl.pallas_call(
        functools.partial(kernel, ns, nt, ny),
        out_shape=(
            pltpu.VMEM((nt, own_n, width), BF16),
            pltpu.VMEM(out_weight.shape, BF16),
            pltpu.VMEM((1, d), F32),
            pltpu.VMEM((own_n, d), BF16),
        ),
        in_specs=[hbm] * 13,
        out_specs=(vmem,) * 4,
        scratch_shapes=[
            pltpu.VMEM((tokens, d), BF16),
            pltpu.VMEM((c_here, d), BF16),
            pltpu.VMEM((kt, d), BF16),
            pltpu.VMEM((kt, d), BF16),
            pltpu.VMEM((kt, d), BF16),
            pltpu.VMEM((d, 3 * width), BF16),
            pltpu.VMEM((d // 2 // 512, nt, 8, 512), F32),
            pltpu.VMEM((nt, 8, d // 8), F32),
            pltpu.VMEM((8, d), F32),
            pltpu.VMEM((tokens, HEAD_DIM), F32),
            pltpu.VMEM((2, UP_ROWS * GRID_W, d), BF16),
            pltpu.VMEM((ny, ns // ny, c_here, 2 * width), BF16),
            pltpu.VMEM((tokens + halo, 2 * width), BF16),
            pltpu.VMEM((tokens, width), BF16),
            pltpu.VMEM((DOWN_ROWS * GRID_W, d), BF16),
            pltpu.VMEM((heads, TABLES + 3, GRID_W, PAIR), F32),
            pltpu.VMEM((heads, tokens, KEYS), F32),
            pltpu.VMEM((heads, tokens, ns // ny * c_here), F32),
            pltpu.VMEM((heads, tokens, 2 * HEAD_DIM), F32),
            pltpu.VMEM((heads, tokens, HEAD_DIM), F32),
            pltpu.VMEM((tokens, width), BF16),
            pltpu.VMEM((2 * WIN_ROWS - 1, heads, PAIR), F32),
            pltpu.VMEM((1, d), F32),
            pltpu.VMEM((1, d), F32),
            pltpu.VMEM((1, d), F32),
            pltpu.VMEM(table.shape, F32),
            sem((12 + d // 2 // 512,)),
            sem((nt - 1,)), sem((nt - 1,)), sem((nt - 1,)), sem((nt - 1,)),
            sem((ns // ny, max(ny - 1, 1))), sem((2, ns)), sem((2, ns)),
            sem((len(HALO),)), sem((len(HALO),)),
            sem((RAW_PARTS, 2 * (nt // CORES))), sem((RAW_PARTS, nt)),
            sem((nt - 1,)), sem((nt - 1,)),
        ],
        compiler_params=pltpu.CompilerParams(
            collective_id=0, has_side_effects=True, vmem_limit_bytes=VMEM_BYTES - tail
        ),
    )(
        cond[None], ctx_cond[None], norm_gain[None], table, latents, context, shift_weight, scale_weight, gate_weight,
        q_weight, k_weight, v_weight, out_weight,
    )
    return pl.pallas_call(
        finish,
        out_shape=jax.ShapeDtypeStruct((own_n, d), BF16),
        in_specs=[vmem] * 4,
        out_specs=hbm,
        scratch_shapes=[pltpu.VMEM((own_n, d), BF16), sem((4,))],
        compiler_params=pltpu.CompilerParams(vmem_limit_bytes=16 * 1024 * 1024),
    )(*parts)


def solution(mesh):
    in_specs = (
        P("sp", None),
        P(),
        P(),
        P("sp", None),
        P(),
        P("tp", None),
        P("tp", None),
        P("tp", None),
        P(None, "tp"),
        P(None, "tp"),
        P(None, "tp"),
        P(),
        P("tp", None, None),
    )
    body = functools.partial(shards, mesh.shape["sp"], mesh.shape["tp"])
    return jax.shard_map(
        body, mesh=mesh, in_specs=in_specs, out_specs=P(("sp", "tp"), None), check_vma=False
    )
```

```python
import functools

import jax
import jax.numpy as jnp
from jax import lax
from jax.experimental import pallas as pl
from jax.experimental.pallas import tpu as pltpu
from jax.sharding import PartitionSpec as P

HEAD_DIM = 128
GRID_W = 64
WIN_ROWS = 8
WIN_COLS = 16
EPS = 1e-06
NEG_BIG = -1e30
F32 = jnp.float32
BF16 = jnp.bfloat16
UP_ROWS = WIN_ROWS // 2
DOWN_ROWS = WIN_ROWS // 2 - 1
PAIR = 2 * GRID_W
KEY_ROWS = WIN_ROWS + 2
KEYS = KEY_ROWS * GRID_W
TABLES = 2 * WIN_ROWS - 2
Z_FIRST = 3
HALO = ((0, 2), (2, 2))
ISSUE = ((), ((0, 0),), (), (), ((1, 0),))
RAW_PARTS = 1
CORES = 2
VMEM_BYTES = 67043328


def dot(a, b):
    return jnp.dot(a, b, preferred_element_type=F32)


def dot_t(a, b):
    return lax.dot_general(a, b, (((1,), (1,)), ((), ())), preferred_element_type=F32)


def wide(x, n):
    return jnp.concatenate([x] * pl.cdiv(n, HEAD_DIM), axis=1)[:, :n]


def kernel(
    ns, nt, ny,
    cond_h, ctx_cond_h, gain_h, table_h,
    lat_h, ctx_h, wsh_h, wsc_h, wg_h, wq_h, wk_h, wv_h, wo_h,
    own, wo, gates, lat_own, y_own,
    lat, ctx, wsh, wsc, wg, wqkv,
    modr, gater, mods, inv, hbuf, ctx_all, kv, q, raw, bias, s_near, s_far, acc, mx, att, lines,
    cond, ctx_cond, gain, table,
    load_sem, mod_s, mod_r, gate_s, gate_r, across_s, along_s, ctx_r, halo_s, halo_r, raw_s, raw_r, head_s, head_r,
):
    sp, tp = lax.axis_index("sp"), lax.axis_index("tp")
    tokens, d = lat.shape
    c_here = ctx.shape[0]
    width = q.shape[1]
    heads = width // HEAD_DIM
    kt = wsh.shape[0]
    rows = tokens // GRID_W
    total_rows = rows * ns
    own_n = tokens // nt
    up_n, down_n = UP_ROWS * GRID_W, DOWN_ROWS * GRID_W
    to_log2 = 1.4426950408889634
    q_scale = HEAD_DIM ** -0.5 * to_log2
    half_d = d // 2
    step = 512

    count = [0]

    def load(s, t, same=None):
        if same is None:
            same = count[0]
            count[0] += 1
        return pltpu.make_async_copy(s, t, load_sem.at[same])

    small = [load(cond_h, cond), load(ctx_cond_h, ctx_cond), load(gain_h, gain), load(table_h, table)]
    mod_loads, mod_slots = [], []
    for n0 in range(0, half_d, step):
        slot_here = count[0]
        mod_slots.append(slot_here)
        count[0] += 1
        mod_loads.append([
            load(s.at[:, pl.ds(k * half_d + n0, step)], t.at[:, pl.ds(k * half_d + n0, step)], slot_here)
            for k in range(2) for s, t in ((wsh_h, wsh), (wsc_h, wsc))
        ])
    ctx_load, lat_load, wg_load = load(ctx_h, ctx), load(lat_h, lat), load(wg_h, wg)
    wk_load = load(wk_h, wqkv.at[:, pl.ds(0, width)])
    wv_load = load(wv_h, wqkv.at[:, pl.ds(width, width)])
    wq_load = load(wq_h, wqkv.at[:, pl.ds(2 * width, width)])
    wo_load = load(wo_h, wo)
    my_rows = pl.ds(pl.multiple_of(tp * own_n, 16), own_n)
    own_load = load(lat_h.at[my_rows], lat_own)
    for c in small + sum(mod_loads, []) + [ctx_load, lat_load]:
        c.start()

    barrier = pltpu.get_barrier_semaphore()

    def greet_tp(o, _):
        pl.semaphore_signal(barrier, inc=1, device_id={"sp": sp, "tp": (tp + o) % nt})
        return 0

    def greet_sp(o, _):
        pl.semaphore_signal(barrier, inc=1, device_id={"sp": (sp + o) % ns, "tp": tp})
        return 0

    lax.fori_loop(1, nt, greet_tp, 0)
    lax.fori_loop(1, ns, greet_sp, 0)

    for c in small:
        c.wait()

    start = pl.multiple_of(tp * kt, 128)
    row = lax.broadcasted_iota(jnp.int32, (8, kt), 0)

    def silu(ref):
        v = ref[:, pl.ds(start, kt)]
        return jnp.broadcast_to(v / (1.0 + jnp.exp(-v)), (8, kt))

    row0_act = silu(cond)
    mixed_act = jnp.where(row % 2 == 0, row0_act, silu(ctx_cond))

    def only(a, keep):
        return jnp.where(keep, a, 0.0).astype(BF16)

    a_sh = [only(mixed_act, (row // 2) == 2 * k) for k in range(2)]
    a_sc = [only(mixed_act, (row // 2) == 2 * k + 1) for k in range(2)]
    def mod_copy(i, o):
        return pltpu.make_async_remote_copy(
            src_ref=modr.at[i, tp], dst_ref=modr.at[i, tp],
            send_sem=mod_s.at[o - 1], recv_sem=mod_r.at[o - 1],
            device_id={"sp": sp, "tp": (tp + o) % nt},
        )

    def each_mod(i, act):
        def one(o, _):
            act(mod_copy(i, o))
            return 0

        lax.fori_loop(1, nt, one, 0)

    chunks = half_d // step
    for i in range(chunks):
        load(wsh_h.at[:, pl.ds(0, 4 * step)], wsh.at[:, pl.ds(0, 4 * step)], mod_slots[i]).wait()
        part = jnp.zeros((8, step), F32)
        for k in range(2):
            cols = pl.ds(k * half_d + i * step, step)
            part = part + dot(a_sh[k], wsh[:, cols])
            part = part + dot(a_sc[k], wsc[:, cols])
        modr[i, tp] = part
        if i == 0:
            pl.semaphore_wait(barrier, nt - 1 + ns - 1)
        each_mod(i, lambda c: c.start())
    quarter = down_n // nt
    piece = quarter // RAW_PARTS
    nx = nt // CORES
    core, xi = tp % CORES, tp // CORES
    has_next, has_prev = sp < ns - 1, sp > 0

    def raw_at(i, t):
        return raw.at[pl.ds(pl.multiple_of(t * quarter, 8) + i * piece, piece)]

    def raw_first(i):
        src = lat_h.at[pl.ds(pl.multiple_of(tp * quarter, 8) + i * piece, piece)]
        return pltpu.make_async_remote_copy(
            src_ref=src, dst_ref=raw_at(i, tp), send_sem=raw_s.at[i, 0], recv_sem=raw_r.at[i, tp],
            device_id={"sp": (sp + ns - 1) % ns, "tp": tp},
        )

    def raw_next(i, t, dest, lane):
        return pltpu.make_async_remote_copy(
            src_ref=raw_at(i, t), dst_ref=raw_at(i, t), send_sem=raw_s.at[i, lane], recv_sem=raw_r.at[i, t],
            device_id={"sp": sp, "tp": dest},
        )

    def raw_x(i, o):
        return raw_next(i, tp, (xi + o) % nx * CORES + core, o)

    def raw_mate(i, o):
        return raw_next(i, (xi + o) % nx * CORES + core, xi * CORES + (core + 1) % CORES, nx + o)

    def raw_got(i, t):
        raw_next(i, t, tp, 0).wait_recv()

    def raw_along(i):
        @pl.when(has_next)
        def _():
            raw_got(i, tp)
            for o in range(1, nx):
                raw_x(i, o).start()
            raw_mate(i, 0).start()

    def raw_over(i):
        @pl.when(has_next)
        def _():
            for o in range(1, nx):
                raw_got(i, (xi + o) % nx * CORES + core)
                raw_mate(i, o).start()

    def raw_done(i):
        @pl.when(has_prev)
        def _():
            raw_first(i).wait_send()

        @pl.when(has_next)
        def _():
            for o in range(nx):
                raw_got(i, (xi + o) % nx * CORES + (core + 1) % CORES)
                raw_mate(i, o).wait_send()
                if o:
                    raw_x(i, o).wait_send()

    @pl.when(has_prev)
    def _():
        for i in range(RAW_PARTS):
            raw_first(i).start()

    for c in [wg_load, wk_load, wv_load, wq_load, wo_load, own_load]:
        c.start()

    def tp_copy(buf, s_sem, r_sem, o):
        return pltpu.make_async_remote_copy(
            src_ref=buf.at[tp], dst_ref=buf.at[tp],
            send_sem=s_sem.at[o - 1], recv_sem=r_sem.at[o - 1],
            device_id={"sp": sp, "tp": (tp + o) % nt},
        )

    qc = lax.broadcasted_iota(jnp.int32, (GRID_W, PAIR), 0)
    lane = lax.broadcasted_iota(jnp.int32, (GRID_W, PAIR), 1)
    kc = lane % GRID_W
    first = jnp.clip(qc - WIN_COLS // 2, 0, GRID_W - WIN_COLS)
    inside = (kc >= first) & (kc < first + WIN_COLS)
    lines[...] = jnp.zeros_like(lines)
    lines[:, :, 0:2 * WIN_COLS - 1] = table[...]
    low_row = WIN_ROWS - 1 - WIN_ROWS // 2
    for h in range(heads):
        for i in range(TABLES):
            near_line = jnp.broadcast_to(lines[i, h:h + 1, :], (GRID_W, PAIR))
            next_line = jnp.broadcast_to(lines[i + 1, h:h + 1, :], (GRID_W, PAIR))
            reach = WIN_COLS - 1
            rolled = pltpu.roll(near_line, PAIR - reach, 1, stride=1, stride_axis=0)
            rolled = rolled + pltpu.roll(next_line, GRID_W - reach, 1, stride=1, stride_axis=0)
            both = jnp.where(inside, rolled * to_log2, NEG_BIG)
            bias[h, i] = both
            if i == low_row - 1:
                bias[h, TABLES] = jnp.where(lane >= GRID_W, both, NEG_BIG)
            if i == low_row + WIN_ROWS - 1:
                bias[h, TABLES + 1] = jnp.where(lane < GRID_W, both, NEG_BIG)
        bias[h, TABLES + 2] = jnp.full((GRID_W, PAIR), NEG_BIG, F32)
    mx[...] = jnp.full_like(mx, NEG_BIG)
    acc[...] = jnp.zeros_like(acc)
    n_keys = kv.shape[0] - tokens - up_n

    @pl.when(sp == ns - 1)
    def _():
        raw[...] = jnp.zeros_like(raw)

    @pl.when(sp == 0)
    def _():
        kv[0:up_n, :] = jnp.zeros((up_n, 2 * width), BF16)

    kv[pl.ds(up_n + tokens + down_n, n_keys - down_n), :] = jnp.zeros((n_keys - down_n, 2 * width), BF16)

    def inv_of(x):
        xf = x.astype(F32)
        return lax.rsqrt(jnp.mean(xf * xf, axis=-1, keepdims=True) + EPS)

    ctx_load.wait()
    ctx_inv = inv_of(ctx[...])
    lat_load.wait()
    for t in range(0, tokens, GRID_W):
        inv[t:t + GRID_W, :] = jnp.broadcast_to(inv_of(lat[t:t + GRID_W, :]), (GRID_W, HEAD_DIM))

    wg_load.wait()
    seg = d // 8
    gp = jnp.zeros((8, seg), F32)
    for j in range(8):
        gp = gp + dot(only(row0_act, row == j), wg[:, pl.ds(j * seg, seg)])
    gater[tp] = gp

    def start_gate(o, _):
        tp_copy(gater, gate_s, gate_r, o).start()
        return 0

    lax.fori_loop(1, nt, start_gate, 0)
    wk_load.wait()
    wv_load.wait()

    each_mod(pl.ds(0, chunks), lambda c: c.wait())
    g = gain[...]
    for i in range(chunks):
        total = modr[i, 0]
        for j in range(1, nt):
            total = total + modr[i, j]
        for k in range(2):
            lo = k * half_d + i * step
            cols = pl.ds(lo, step)
            gk = g[:, lo:lo + step]
            mods[0:1, cols] = gk * (1.0 + total[4 * k + 2:4 * k + 3])
            mods[1:2, cols] = total[4 * k:4 * k + 1]
            mods[2:3, cols] = gk * (1.0 + total[4 * k + 3:4 * k + 4])
            mods[3:4, cols] = total[4 * k + 1:4 * k + 2]

    ctx_hid = (ctx[...].astype(F32) * ctx_inv * mods[2:3, :] + mods[3:4, :]).astype(BF16)
    ctx_all[sp % ny, sp // ny] = dot(ctx_hid, wqkv[:, 0:2 * width]).astype(BF16)

    nz = ns // ny
    zi, yi = sp // ny, sp % ny

    cut = max(Z_FIRST * width // 2 // HEAD_DIM, 1) * HEAD_DIM

    def ctx_copy(part, block, dest, send_sem):
        cols = (pl.ds(0, cut), pl.ds(cut, 2 * width - cut), pl.ds(0, 2 * width))[part]
        ref = ctx_all.at[block % ny, block // ny, :, cols]
        return pltpu.make_async_remote_copy(
            src_ref=ref, dst_ref=ref, send_sem=send_sem, recv_sem=ctx_r.at[part % 2, block],
            device_id={"sp": dest, "tp": tp},
        )

    def across(part, zb, act):
        def one(o, _):
            act(ctx_copy(part, zb * ny + yi, zi * ny + (yi + o) % ny, across_s.at[zb, o - 1]))
            return 0

        lax.fori_loop(1, ny, one, 0)

    def upward(part, block, act):
        @pl.when(zi < nz - 1)
        def _():
            act(ctx_copy(part, block, sp + ny, along_s.at[0, block]))

    def downward(part, block, act):
        @pl.when(zi > 0)
        def _():
            act(ctx_copy(part, block, sp - ny, along_s.at[1, block]))

    def go(c):
        c.start()

    def sent(c):
        c.wait_send()

    def arrived(part, block):
        ctx_copy(part, block, sp, along_s.at[0, block]).wait_recv()

    def beside():
        def one(o, _):
            block = zi * ny + (yi + o) % ny
            arrived(1, block)
            upward(1, block, go)
            downward(1, block, go)
            return 0

        lax.fori_loop(1, ny, one, 0)

    def pass_first(zb, forward):
        block = zb * ny + yi
        arrived(0, block)
        forward(0, block, go)
        across(0, zb, go)

    def pass_second(zb, forward):
        def one(o, _):
            other = zb * ny + (yi + o) % ny
            arrived(1, other)
            forward(1, other, go)
            return 0

        lax.fori_loop(0, ny, one, 0)

    def relay_down(k, pass_on):
        @pl.when(zi + k < nz)
        def _():
            pass_on(zi + k, downward)

    def relay_up(k, pass_on):
        @pl.when(zi - k >= 0)
        def _():
            pass_on(zi - k, upward)

    def relay(k, pass_on):
        relay_down(k, pass_on)
        relay_up(k, pass_on)

    across(1, zi, go)
    for part in range(2):
        upward(part, sp, go)
        downward(part, sp, go)
    across(0, zi, go)

    def halo(i):
        lo, n = HALO[i]
        return pltpu.make_async_remote_copy(
            src_ref=kv.at[pl.ds(tokens + lo * GRID_W, n * GRID_W)],
            dst_ref=kv.at[pl.ds(lo * GRID_W, n * GRID_W)],
            send_sem=halo_s.at[i], recv_sem=halo_r.at[i],
            device_id={"sp": (sp + 1) % ns, "tp": tp},
        )

    def send_halo(point):
        for i, which in ISSUE[point]:
            turn = (yi >= 0, yi == ny - 1, yi < ny - 1)[which]
            pl.when(has_next & turn)(lambda c=halo(i): c.start())

    wq_load.wait()
    rest = (tokens - up_n) // 2
    spans = [(tokens - up_n, up_n), (0, rest), (rest, rest)]

    def modulate(x, scale):
        return (x.astype(F32) * scale * mods[0:1, :] + mods[1:2, :]).astype(BF16)

    def hidden(i):
        lo, n = spans[i]
        hbuf[i % 2, 0:n, :] = modulate(lat[lo:lo + n, :], wide(inv[lo:lo + n, :], d))

    hidden(0)
    for i, (lo, n) in enumerate(spans):
        r = dot(hbuf[i % 2, 0:n, :], wqkv[...])
        kv[lo + up_n:lo + up_n + n, :] = r[:, :2 * width].astype(BF16)
        q[lo:lo + n, :] = (r[:, 2 * width:] * q_scale).astype(BF16)
        if i + 1 < len(spans):
            hidden(i + 1)
        if i == 0:
            send_halo(0)
            raw_along(0)
        if i == 1:
            beside()
            send_halo(1)

    half_t = nt // 2
    my_half = tp // half_t
    base_row = sp * rows
    ones = jnp.ones((1, HEAD_DIM), BF16)

    def with_ones(v):
        return jnp.concatenate([v, jnp.broadcast_to(ones, v.shape)], axis=1)

    def window(r):
        grid_row = base_row + r
        s0 = jnp.clip(grid_row - WIN_ROWS // 2, 0, total_rows - WIN_ROWS)
        s1 = jnp.clip(grid_row + 1 - WIN_ROWS // 2, 0, total_rows - WIN_ROWS)
        win = pl.ds(pl.multiple_of((s0 - base_row + UP_ROWS) * GRID_W, GRID_W), KEYS)
        return grid_row, s0, s1, win

    def near_scores(r, h):
        grid_row, s0, s1, win = window(r)
        i0 = s0 - grid_row + WIN_ROWS - 1
        i1 = i0 - 1
        moved = s1 > s0
        lo = h * HEAD_DIM
        t = r * GRID_W
        s = dot_t(q[t:t + PAIR, lo:lo + HEAD_DIM], kv[win, lo:lo + HEAD_DIM])
        b0 = [bias[h, i0 + 2 * k] for k in range(WIN_ROWS // 2)]
        ids = [jnp.where(moved, TABLES, i1)]
        ids += [jnp.where(moved, i1 + 2 * k, i1 + 2 * k) for k in range(1, WIN_ROWS // 2)]
        ids += [jnp.where(moved, TABLES + 1, TABLES + 2)]
        b1 = [bias[h, i] for i in ids]
        x0 = s[:GRID_W, :WIN_ROWS * GRID_W] + jnp.concatenate(b0, axis=1)
        x1 = s[GRID_W:, :] + jnp.concatenate(b1, axis=1)
        s_near[h, t:t + GRID_W, 0:WIN_ROWS * GRID_W] = x0
        s_near[h, t + GRID_W:t + PAIR, :] = x1
        m = jnp.concatenate([jnp.max(x0, axis=-1, keepdims=True), jnp.max(x1, axis=-1, keepdims=True)], axis=0)
        return jnp.broadcast_to(m, (PAIR, HEAD_DIM))

    def near_values(r, h, m):
        win = window(r)[3]
        lo = h * HEAD_DIM
        t = r * GRID_W
        old = mx[h, t:t + PAIR, :]
        m = jnp.maximum(m, old)
        w = jnp.exp2(old - m)
        n0 = WIN_ROWS * GRID_W
        e0 = jnp.exp2(s_near[h, t:t + GRID_W, 0:n0] - wide(m[:GRID_W], n0)).astype(BF16)
        e1 = jnp.exp2(s_near[h, t + GRID_W:t + PAIR, :] - wide(m[GRID_W:], KEYS)).astype(BF16)
        e0 = jnp.concatenate([e0, jnp.zeros((GRID_W, KEYS - n0), BF16)], axis=1)
        p = jnp.concatenate([e0, e1], axis=0)
        o = dot(p, with_ones(kv[win, width + lo:width + lo + HEAD_DIM]))
        mx[h, t:t + PAIR, :] = m
        acc[h, t:t + PAIR, :] = acc[h, t:t + PAIR, :] * wide(w, 2 * HEAD_DIM) + o

    def near(pairs):
        units = [(r, h) for r in pairs for h in range(heads)]
        ms = [near_scores(r, h) for r, h in units]
        for (r, h), m in zip(units, ms):
            near_values(r, h, m)

    def flat(x):
        n = x.shape[0] * c_here
        if c_here % 16:
            return x.astype(F32).reshape(n, HEAD_DIM).astype(BF16)
        return x.reshape(n, HEAD_DIM)

    def far_scores(t, col, zs, h):
        lo = h * HEAD_DIM
        s = dot_t(q[t, lo:lo + HEAD_DIM], flat(ctx_all[col, zs, :, lo:lo + HEAD_DIM]))
        s_far[h, t, 0:s.shape[1]] = s
        return jnp.broadcast_to(jnp.max(s, axis=-1, keepdims=True), (own_n, HEAD_DIM))

    def far_values(t, col, zs, h, m, last):
        lo = width + h * HEAD_DIM
        v = flat(ctx_all[col, zs, :, lo:lo + HEAD_DIM])
        old = mx[h, t, :]
        m = jnp.maximum(m, old)
        w = jnp.exp2(old - m)
        n = v.shape[0]
        e = jnp.exp2(s_far[h, t, 0:n] - wide(m, n)).astype(BF16)
        o = acc[h, t, :] * wide(w, 2 * HEAD_DIM) + dot(e, with_ones(v))
        if last:
            lo = h * HEAD_DIM
            att[t, lo:lo + HEAD_DIM] = (o[:, :HEAD_DIM] / o[:, HEAD_DIM:]).astype(BF16)
        else:
            mx[h, t, :] = m
            acc[h, t, :] = o

    def far(parts, o, zs, last):
        col = (yi + o) % ny
        units = [(pl.ds(pl.multiple_of(p * own_n, 16), own_n), h) for p in parts for h in range(heads)]
        ms = [far_scores(t, col, zs, h) for t, h in units]
        for (t, h), m in zip(units, ms):
            far_values(t, col, zs, h, m, last)

    everything = pl.ds(0, nz)

    relay(1, pass_first)
    for i in range(1, RAW_PARTS):
        raw_along(i)
    near(range(UP_ROWS, rows - UP_ROWS, 2))
    relay(1, pass_second)
    send_halo(2)
    if nz > 2:
        relay(2, pass_first)
    send_halo(3)
    for i in range(RAW_PARTS):
        raw_over(i)
    if nz > 2:
        relay(2, pass_second)
    send_halo(4)
    for i in range(RAW_PARTS):
        raw_done(i)
    hbuf[0, 0:down_n, :] = modulate(raw[...], inv_of(raw[...]))
    below = dot(hbuf[0, 0:down_n, :], wqkv[:, 0:2 * width])
    kv[up_n + tokens:up_n + tokens + down_n, :] = below.astype(BF16)
    up_pairs, down_pairs = range(0, UP_ROWS, 2), range(rows - UP_ROWS, rows, 2)

    def halo_near():
        for i in range(len(HALO)):
            pl.when(has_prev)(lambda c=halo(i): c.wait_recv())
        near(up_pairs)

    if nz > 3:
        relay_down(3, pass_first)
    pl.when(my_half == 0)(lambda: near(down_pairs))
    pl.when((my_half == 1) & (sp == 0))(lambda: near(up_pairs))
    if nz > 3:
        relay_up(3, pass_first)
    if nz > 3:
        relay(3, pass_second)

    def late_relay(k, _):
        relay(k, pass_first)
        relay(k, pass_second)
        return 0

    lax.fori_loop(4, nz, late_relay, 0)
    theirs = [(1 - my_half) * half_t + j for j in range(half_t)]
    ours = [my_half * half_t + (tp + o) % half_t for o in range(half_t)]
    low = zi < nz - nz // 2
    z_last = jnp.where(low, nz - 1, 0)
    z_rest = pl.ds(jnp.where(low, 0, 1), nz - 1)

    def others(zb):
        def other(o, _):
            arrived(0, zb * ny + (yi + o) % ny)
            return 0

        lax.fori_loop(1, ny, other, 0)

    def middle(parts, zs):
        lax.fori_loop(1, ny - 1, lambda o, c: (far(parts, o, zs, False), c)[1], 0)

    def far_own(parts):
        if ny > 1:
            far(parts, 0, everything, False)

    def far_rest(parts):
        if nz > 1:
            middle(parts, z_rest)
            far(parts, ny - 1, z_rest, False)

    far_own(theirs)
    for k in range(nz - 1):
        others(z_rest.start + k)
    far_rest(theirs)
    pl.when((my_half == 1) & (sp > 0))(halo_near)
    others(z_last)
    middle(theirs, pl.ds(z_last, 1))

    def settle_row(zb, _):
        pl.when(zb == zi)(lambda: across(2, zb, sent))
        pl.when(zb != zi)(lambda: across(0, zb, sent))

        @pl.when(zb <= zi)
        def _():
            upward(2, zb * ny + yi, sent)

        @pl.when(zb >= zi)
        def _():
            downward(2, zb * ny + yi, sent)

        def column(o, _):
            block = zb * ny + (yi + o) % ny

            @pl.when(zb <= zi)
            def _():
                upward(1, block, sent)

            @pl.when(zb >= zi)
            def _():
                downward(1, block, sent)

            return 0

        lax.fori_loop(1, ny, column, 0)
        return 0

    def head_copy(src, dst):
        return pltpu.make_async_remote_copy(
            src_ref=att.at[pl.ds(pl.multiple_of(dst * own_n, 16), own_n)], dst_ref=own.at[src],
            send_sem=head_s.at[(dst - src + nt - 1) % nt], recv_sem=head_r.at[(dst - src + nt - 1) % nt],
            device_id={"sp": sp, "tp": dst},
        )

    for p in theirs:
        far([p], ny - 1, pl.ds(z_last, 1), True)
        head_copy(tp, p).start()
    pl.when(my_half == 0)(halo_near)
    pl.when(my_half == 1)(lambda: near(down_pairs))
    far_own(ours)
    far_rest(ours)
    middle(ours, pl.ds(z_last, 1))
    far(ours, ny - 1, pl.ds(z_last, 1), True)
    for p in ours[1:]:
        head_copy(tp, p).start()
    for i in range(len(HALO)):
        pl.when(has_next)(lambda c=halo(i): c.wait_send())
    lax.fori_loop(0, nz, settle_row, 0)

    def wait_gate(o, _):
        tp_copy(gater, gate_s, gate_r, o).wait()
        return 0

    lax.fori_loop(1, nt, wait_gate, 0)
    gsum = gater[0]
    for i in range(1, nt):
        gsum = gsum + gater[i]
    gates[...] = jnp.concatenate([gsum[j:j + 1] for j in range(8)], axis=1)
    wo_load.wait()
    own_load.wait()

    def taken(p):
        head_copy(tp, p).wait_send()
        head_copy(p, tp).wait_recv()

    def part_of(p):
        return pl.ds(pl.multiple_of(p * width, HEAD_DIM), width)

    for n0 in range(0, d, step):
        y_own[:, n0:n0 + step] = dot(att[my_rows, :], wo[part_of(tp), n0:n0 + step])
    for p in ours[1:]:
        taken(p)
        for n0 in range(0, d, step):
            y_own[:, n0:n0 + step] += dot(own[p], wo[part_of(p), n0:n0 + step])
    for p in theirs:
        taken(p)


def finish(own, wo, gates, lat_own, y_own, out, buf, sem):
    nt, _, width = own.shape
    d = wo.shape[1]
    step = d // 4
    half_t = nt // 2
    other = (1 - lax.axis_index("tp") // half_t) * half_t
    a = jnp.concatenate([own[other + i] for i in range(half_t)], axis=1)
    rows = pl.ds(pl.multiple_of(other * width, HEAD_DIM), half_t * width)
    copies = []
    for i in range(4):
        cols = pl.ds(i * step, step)
        y = y_own[:, cols] + dot(a, wo[rows, cols])
        buf[:, cols] = (lat_own[:, cols].astype(F32) + gates[:, cols] * y).astype(BF16)
        copies.append(pltpu.make_async_copy(buf.at[:, cols], out.at[:, cols], sem.at[i]))
        copies[-1].start()
    for c in copies:
        c.wait()


def shards(
    ns, nt,
    latents, cond, ctx_cond, context, norm_gain, shift_weight, scale_weight, gate_weight,
    q_weight, k_weight, v_weight, out_weight, rel_bias,
):
    tokens, d = latents.shape
    c_here = context.shape[0]
    kt = shift_weight.shape[0]
    width = q_weight.shape[1]
    heads = width // HEAD_DIM
    own_n = tokens // nt
    table = jnp.transpose(rel_bias, (1, 0, 2))
    ny = 1
    while ns % (2 * ny) == 0 and 4 * ny * ny <= ns:
        ny *= 2
    halo = (UP_ROWS + DOWN_ROWS + 1) * GRID_W
    vmem = pl.BlockSpec(memory_space=pltpu.VMEM)
    hbm = pl.BlockSpec(memory_space=pltpu.HBM)
    sem = pltpu.SemaphoreType.DMA
    tail = 8 * 1024 * 1024
    parts = pl.pallas_call(
        functools.partial(kernel, ns, nt, ny),
        out_shape=(
            pltpu.VMEM((nt, own_n, width), BF16),
            pltpu.VMEM(out_weight.shape, BF16),
            pltpu.VMEM((1, d), F32),
            pltpu.VMEM((own_n, d), BF16),
            pltpu.VMEM((own_n, d), F32),
        ),
        in_specs=[hbm] * 13,
        out_specs=(vmem,) * 5,
        scratch_shapes=[
            pltpu.VMEM((tokens, d), BF16),
            pltpu.VMEM((c_here, d), BF16),
            pltpu.VMEM((kt, d), BF16),
            pltpu.VMEM((kt, d), BF16),
            pltpu.VMEM((kt, d), BF16),
            pltpu.VMEM((d, 3 * width), BF16),
            pltpu.VMEM((d // 2 // 512, nt, 8, 512), F32),
            pltpu.VMEM((nt, 8, d // 8), F32),
            pltpu.VMEM((8, d), F32),
            pltpu.VMEM((tokens, HEAD_DIM), F32),
            pltpu.VMEM((2, UP_ROWS * GRID_W, d), BF16),
            pltpu.VMEM((ny, ns // ny, c_here, 2 * width), BF16),
            pltpu.VMEM((tokens + halo, 2 * width), BF16),
            pltpu.VMEM((tokens, width), BF16),
            pltpu.VMEM((DOWN_ROWS * GRID_W, d), BF16),
            pltpu.VMEM((heads, TABLES + 3, GRID_W, PAIR), F32),
            pltpu.VMEM((heads, tokens, KEYS), F32),
            pltpu.VMEM((heads, tokens, ns // ny * c_here), F32),
            pltpu.VMEM((heads, tokens, 2 * HEAD_DIM), F32),
            pltpu.VMEM((heads, tokens, HEAD_DIM), F32),
            pltpu.VMEM((tokens, width), BF16),
            pltpu.VMEM((2 * WIN_ROWS - 1, heads, PAIR), F32),
            pltpu.VMEM((1, d), F32),
            pltpu.VMEM((1, d), F32),
            pltpu.VMEM((1, d), F32),
            pltpu.VMEM(table.shape, F32),
            sem((12 + d // 2 // 512,)),
            sem((nt - 1,)), sem((nt - 1,)), sem((nt - 1,)), sem((nt - 1,)),
            sem((ns // ny, max(ny - 1, 1))), sem((2, ns)), sem((2, ns)),
            sem((len(HALO),)), sem((len(HALO),)),
            sem((RAW_PARTS, 2 * (nt // CORES))), sem((RAW_PARTS, nt)),
            sem((nt - 1,)), sem((nt - 1,)),
        ],
        compiler_params=pltpu.CompilerParams(
            collective_id=0, has_side_effects=True, vmem_limit_bytes=VMEM_BYTES - tail
        ),
    )(
        cond[None], ctx_cond[None], norm_gain[None], table, latents, context, shift_weight, scale_weight, gate_weight,
        q_weight, k_weight, v_weight, out_weight,
    )
    return pl.pallas_call(
        finish,
        out_shape=jax.ShapeDtypeStruct((own_n, d), BF16),
        in_specs=[vmem] * 5,
        out_specs=hbm,
        scratch_shapes=[pltpu.VMEM((own_n, d), BF16), sem((4,))],
        compiler_params=pltpu.CompilerParams(vmem_limit_bytes=16 * 1024 * 1024),
    )(*parts)


def solution(mesh):
    in_specs = (
        P("sp", None),
        P(),
        P(),
        P("sp", None),
        P(),
        P("tp", None),
        P("tp", None),
        P("tp", None),
        P(None, "tp"),
        P(None, "tp"),
        P(None, "tp"),
        P(),
        P("tp", None, None),
    )
    body = functools.partial(shards, mesh.shape["sp"], mesh.shape["tp"])
    return jax.shard_map(
        body, mesh=mesh, in_specs=in_specs, out_specs=P(("sp", "tp"), None), check_vma=False
    )
```

```python
import functools

import jax
import jax.numpy as jnp
from jax import lax
from jax.experimental import pallas as pl
from jax.experimental.pallas import tpu as pltpu
from jax.sharding import PartitionSpec as P

HEAD_DIM = 128
GRID_W = 64
WIN_ROWS = 8
WIN_COLS = 16
EPS = 1e-06
NEG_BIG = -1e30
F32 = jnp.float32
BF16 = jnp.bfloat16
UP_ROWS = WIN_ROWS // 2
DOWN_ROWS = WIN_ROWS // 2 - 1
PAIR = 2 * GRID_W
KEY_ROWS = WIN_ROWS + 2
KEYS = KEY_ROWS * GRID_W
TABLES = 2 * WIN_ROWS - 2
Z_FIRST = 3
HALO = ((0, 2), (2, 2))
ISSUE = ((), ((0, 0),), (), (), ((1, 0),))
RAW_PARTS = 1
CORES = 2
VMEM_BYTES = 67043328


def dot(a, b):
    return jnp.dot(a, b, preferred_element_type=F32)


def dot_t(a, b):
    return lax.dot_general(a, b, (((1,), (1,)), ((), ())), preferred_element_type=F32)


def wide(x, n):
    return jnp.concatenate([x] * pl.cdiv(n, HEAD_DIM), axis=1)[:, :n]


def kernel(
    ns, nt, ny,
    cond_h, ctx_cond_h, gain_h, table_h,
    lat_h, ctx_h, wsh_h, wsc_h, wg_h, wq_h, wk_h, wv_h, wo_h,
    own, wo, gates, lat_own, y_own,
    lat, ctx, wsh, wsc, wg, wqkv,
    modr, gater, mods, inv, hbuf, ctx_all, kv, q, raw, bias, s_near, s_far, acc, mx, att, lines,
    cond, ctx_cond, gain, table,
    load_sem, mod_s, mod_r, gate_s, gate_r, across_s, along_s, ctx_r, halo_s, halo_r, raw_s, raw_r, head_s, head_r,
):
    sp, tp = lax.axis_index("sp"), lax.axis_index("tp")
    tokens, d = lat.shape
    c_here = ctx.shape[0]
    width = q.shape[1]
    heads = width // HEAD_DIM
    kt = wsh.shape[0]
    rows = tokens // GRID_W
    total_rows = rows * ns
    own_n = tokens // nt
    up_n, down_n = UP_ROWS * GRID_W, DOWN_ROWS * GRID_W
    to_log2 = 1.4426950408889634
    q_scale = HEAD_DIM ** -0.5 * to_log2
    half_d = d // 2
    step = 512

    count = [0]

    def load(s, t, same=None):
        if same is None:
            same = count[0]
            count[0] += 1
        return pltpu.make_async_copy(s, t, load_sem.at[same])

    small = [load(cond_h, cond), load(ctx_cond_h, ctx_cond), load(gain_h, gain), load(table_h, table)]
    mod_loads, mod_slots = [], []
    for n0 in range(0, half_d, step):
        slot_here = count[0]
        mod_slots.append(slot_here)
        count[0] += 1
        mod_loads.append([
            load(s.at[:, pl.ds(k * half_d + n0, step)], t.at[:, pl.ds(k * half_d + n0, step)], slot_here)
            for k in range(2) for s, t in ((wsh_h, wsh), (wsc_h, wsc))
        ])
    ctx_load, lat_load, wg_load = load(ctx_h, ctx), load(lat_h, lat), load(wg_h, wg)
    wk_load = load(wk_h, wqkv.at[:, pl.ds(0, width)])
    wv_load = load(wv_h, wqkv.at[:, pl.ds(width, width)])
    wq_load = load(wq_h, wqkv.at[:, pl.ds(2 * width, width)])
    wo_load = load(wo_h, wo)
    my_rows = pl.ds(pl.multiple_of(tp * own_n, 16), own_n)
    own_load = load(lat_h.at[my_rows], lat_own)
    for c in small + sum(mod_loads, []) + [ctx_load, lat_load]:
        c.start()

    barrier = pltpu.get_barrier_semaphore()

    def greet_tp(o, _):
        pl.semaphore_signal(barrier, inc=1, device_id={"sp": sp, "tp": (tp + o) % nt})
        return 0

    def greet_sp(o, _):
        pl.semaphore_signal(barrier, inc=1, device_id={"sp": (sp + o) % ns, "tp": tp})
        return 0

    lax.fori_loop(1, nt, greet_tp, 0)
    lax.fori_loop(1, ns, greet_sp, 0)

    for c in small:
        c.wait()

    start = pl.multiple_of(tp * kt, 128)
    row = lax.broadcasted_iota(jnp.int32, (8, kt), 0)

    def silu(ref):
        v = ref[:, pl.ds(start, kt)]
        return jnp.broadcast_to(v / (1.0 + jnp.exp(-v)), (8, kt))

    row0_act = silu(cond)
    mixed_act = jnp.where(row % 2 == 0, row0_act, silu(ctx_cond))

    def only(a, keep):
        return jnp.where(keep, a, 0.0).astype(BF16)

    a_sh = [only(mixed_act, (row // 2) == 2 * k) for k in range(2)]
    a_sc = [only(mixed_act, (row // 2) == 2 * k + 1) for k in range(2)]
    def mod_copy(i, o):
        return pltpu.make_async_remote_copy(
            src_ref=modr.at[i, tp], dst_ref=modr.at[i, tp],
            send_sem=mod_s.at[o - 1], recv_sem=mod_r.at[o - 1],
            device_id={"sp": sp, "tp": (tp + o) % nt},
        )

    def each_mod(i, act):
        def one(o, _):
            act(mod_copy(i, o))
            return 0

        lax.fori_loop(1, nt, one, 0)

    chunks = half_d // step
    for i in range(chunks):
        load(wsh_h.at[:, pl.ds(0, 4 * step)], wsh.at[:, pl.ds(0, 4 * step)], mod_slots[i]).wait()
        part = jnp.zeros((8, step), F32)
        for k in range(2):
            cols = pl.ds(k * half_d + i * step, step)
            part = part + dot(a_sh[k], wsh[:, cols])
            part = part + dot(a_sc[k], wsc[:, cols])
        modr[i, tp] = part
        if i == 0:
            pl.semaphore_wait(barrier, nt - 1 + ns - 1)
        each_mod(i, lambda c: c.start())
    quarter = down_n // nt
    piece = quarter // RAW_PARTS
    nx = nt // CORES
    core, xi = tp % CORES, tp // CORES
    has_next, has_prev = sp < ns - 1, sp > 0

    def raw_at(i, t):
        return raw.at[pl.ds(pl.multiple_of(t * quarter, 8) + i * piece, piece)]

    def raw_first(i):
        src = lat_h.at[pl.ds(pl.multiple_of(tp * quarter, 8) + i * piece, piece)]
        return pltpu.make_async_remote_copy(
            src_ref=src, dst_ref=raw_at(i, tp), send_sem=raw_s.at[i, 0], recv_sem=raw_r.at[i, tp],
            device_id={"sp": (sp + ns - 1) % ns, "tp": tp},
        )

    def raw_next(i, t, dest, lane):
        return pltpu.make_async_remote_copy(
            src_ref=raw_at(i, t), dst_ref=raw_at(i, t), send_sem=raw_s.at[i, lane], recv_sem=raw_r.at[i, t],
            device_id={"sp": sp, "tp": dest},
        )

    def raw_x(i, o):
        return raw_next(i, tp, (xi + o) % nx * CORES + core, o)

    def raw_mate(i, o):
        return raw_next(i, (xi + o) % nx * CORES + core, xi * CORES + (core + 1) % CORES, nx + o)

    def raw_got(i, t):
        raw_next(i, t, tp, 0).wait_recv()

    def raw_along(i):
        @pl.when(has_next)
        def _():
            raw_got(i, tp)
            for o in range(1, nx):
                raw_x(i, o).start()
            raw_mate(i, 0).start()

    def raw_over(i):
        @pl.when(has_next)
        def _():
            for o in range(1, nx):
                raw_got(i, (xi + o) % nx * CORES + core)
                raw_mate(i, o).start()

    def raw_done(i):
        @pl.when(has_prev)
        def _():
            raw_first(i).wait_send()

        @pl.when(has_next)
        def _():
            for o in range(nx):
                raw_got(i, (xi + o) % nx * CORES + (core + 1) % CORES)
                raw_mate(i, o).wait_send()
                if o:
                    raw_x(i, o).wait_send()

    @pl.when(has_prev)
    def _():
        for i in range(RAW_PARTS):
            raw_first(i).start()

    for c in [wg_load, wk_load, wv_load, wq_load, wo_load, own_load]:
        c.start()

    def tp_copy(buf, s_sem, r_sem, o):
        return pltpu.make_async_remote_copy(
            src_ref=buf.at[tp], dst_ref=buf.at[tp],
            send_sem=s_sem.at[o - 1], recv_sem=r_sem.at[o - 1],
            device_id={"sp": sp, "tp": (tp + o) % nt},
        )

    qc = lax.broadcasted_iota(jnp.int32, (GRID_W, PAIR), 0)
    lane = lax.broadcasted_iota(jnp.int32, (GRID_W, PAIR), 1)
    kc = lane % GRID_W
    first = jnp.clip(qc - WIN_COLS // 2, 0, GRID_W - WIN_COLS)
    inside = (kc >= first) & (kc < first + WIN_COLS)
    lines[...] = jnp.zeros_like(lines)
    lines[:, :, 0:2 * WIN_COLS - 1] = table[...]
    low_row = WIN_ROWS - 1 - WIN_ROWS // 2
    for h in range(heads):
        for i in range(TABLES):
            near_line = jnp.broadcast_to(lines[i, h:h + 1, :], (GRID_W, PAIR))
            next_line = jnp.broadcast_to(lines[i + 1, h:h + 1, :], (GRID_W, PAIR))
            reach = WIN_COLS - 1
            rolled = pltpu.roll(near_line, PAIR - reach, 1, stride=1, stride_axis=0)
            rolled = rolled + pltpu.roll(next_line, GRID_W - reach, 1, stride=1, stride_axis=0)
            both = jnp.where(inside, rolled * to_log2, NEG_BIG)
            bias[h, i] = both
            if i == low_row - 1:
                bias[h, TABLES] = jnp.where(lane >= GRID_W, both, NEG_BIG)
            if i == low_row + WIN_ROWS - 1:
                bias[h, TABLES + 1] = jnp.where(lane < GRID_W, both, NEG_BIG)
        bias[h, TABLES + 2] = jnp.full((GRID_W, PAIR), NEG_BIG, F32)
    mx[...] = jnp.full_like(mx, NEG_BIG)
    acc[...] = jnp.zeros_like(acc)
    n_keys = kv.shape[0] - tokens - up_n

    @pl.when(sp == ns - 1)
    def _():
        raw[...] = jnp.zeros_like(raw)

    @pl.when(sp == 0)
    def _():
        kv[0:up_n, :] = jnp.zeros((up_n, 2 * width), BF16)

    kv[pl.ds(up_n + tokens + down_n, n_keys - down_n), :] = jnp.zeros((n_keys - down_n, 2 * width), BF16)

    def inv_of(x):
        xf = x.astype(F32)
        return lax.rsqrt(jnp.mean(xf * xf, axis=-1, keepdims=True) + EPS)

    ctx_load.wait()
    ctx_inv = inv_of(ctx[...])
    lat_load.wait()
    for t in range(0, tokens, GRID_W):
        inv[t:t + GRID_W, :] = jnp.broadcast_to(inv_of(lat[t:t + GRID_W, :]), (GRID_W, HEAD_DIM))

    wg_load.wait()
    seg = d // 8
    gp = jnp.zeros((8, seg), F32)
    for j in range(8):
        gp = gp + dot(only(row0_act, row == j), wg[:, pl.ds(j * seg, seg)])
    gater[tp] = gp

    def start_gate(o, _):
        tp_copy(gater, gate_s, gate_r, o).start()
        return 0

    lax.fori_loop(1, nt, start_gate, 0)
    wk_load.wait()
    wv_load.wait()

    each_mod(pl.ds(0, chunks), lambda c: c.wait())
    g = gain[...]
    for i in range(chunks):
        total = modr[i, 0]
        for j in range(1, nt):
            total = total + modr[i, j]
        for k in range(2):
            lo = k * half_d + i * step
            cols = pl.ds(lo, step)
            gk = g[:, lo:lo + step]
            mods[0:1, cols] = gk * (1.0 + total[4 * k + 2:4 * k + 3])
            mods[1:2, cols] = total[4 * k:4 * k + 1]
            mods[2:3, cols] = gk * (1.0 + total[4 * k + 3:4 * k + 4])
            mods[3:4, cols] = total[4 * k + 1:4 * k + 2]

    ctx_hid = (ctx[...].astype(F32) * ctx_inv * mods[2:3, :] + mods[3:4, :]).astype(BF16)
    ctx_all[sp % ny, sp // ny] = dot(ctx_hid, wqkv[:, 0:2 * width]).astype(BF16)

    nz = ns // ny
    zi, yi = sp // ny, sp % ny

    cut = max(Z_FIRST * width // 2 // HEAD_DIM, 1) * HEAD_DIM

    def ctx_copy(part, block, dest, send_sem):
        cols = (pl.ds(0, cut), pl.ds(cut, 2 * width - cut), pl.ds(0, 2 * width))[part]
        ref = ctx_all.at[block % ny, block // ny, :, cols]
        return pltpu.make_async_remote_copy(
            src_ref=ref, dst_ref=ref, send_sem=send_sem, recv_sem=ctx_r.at[part % 2, block],
            device_id={"sp": dest, "tp": tp},
        )

    def across(part, zb, act):
        def one(o, _):
            act(ctx_copy(part, zb * ny + yi, zi * ny + (yi + o) % ny, across_s.at[zb, o - 1]))
            return 0

        lax.fori_loop(1, ny, one, 0)

    def upward(part, block, act):
        @pl.when(zi < nz - 1)
        def _():
            act(ctx_copy(part, block, sp + ny, along_s.at[0, block]))

    def downward(part, block, act):
        @pl.when(zi > 0)
        def _():
            act(ctx_copy(part, block, sp - ny, along_s.at[1, block]))

    def go(c):
        c.start()

    def sent(c):
        c.wait_send()

    def arrived(part, block):
        ctx_copy(part, block, sp, along_s.at[0, block]).wait_recv()

    def beside():
        def one(o, _):
            block = zi * ny + (yi + o) % ny
            arrived(1, block)
            upward(1, block, go)
            downward(1, block, go)
            return 0

        lax.fori_loop(1, ny, one, 0)

    def pass_first(zb, forward):
        block = zb * ny + yi
        arrived(0, block)
        forward(0, block, go)
        across(0, zb, go)

    def pass_second(zb, forward):
        def one(o, _):
            other = zb * ny + (yi + o) % ny
            arrived(1, other)
            forward(1, other, go)
            return 0

        lax.fori_loop(0, ny, one, 0)

    def relay_down(k, pass_on):
        @pl.when(zi + k < nz)
        def _():
            pass_on(zi + k, downward)

    def relay_up(k, pass_on):
        @pl.when(zi - k >= 0)
        def _():
            pass_on(zi - k, upward)

    def relay(k, pass_on):
        relay_down(k, pass_on)
        relay_up(k, pass_on)

    across(1, zi, go)
    for part in range(2):
        upward(part, sp, go)
        downward(part, sp, go)
    across(0, zi, go)

    def halo(i):
        lo, n = HALO[i]
        return pltpu.make_async_remote_copy(
            src_ref=kv.at[pl.ds(tokens + lo * GRID_W, n * GRID_W)],
            dst_ref=kv.at[pl.ds(lo * GRID_W, n * GRID_W)],
            send_sem=halo_s.at[i], recv_sem=halo_r.at[i],
            device_id={"sp": (sp + 1) % ns, "tp": tp},
        )

    def send_halo(point):
        for i, which in ISSUE[point]:
            turn = (yi >= 0, yi == ny - 1, yi < ny - 1)[which]
            pl.when(has_next & turn)(lambda c=halo(i): c.start())

    wq_load.wait()
    rest = (tokens - up_n) // 2
    spans = [(tokens - up_n, up_n), (0, rest), (rest, rest)]

    def modulate(x, scale):
        return (x.astype(F32) * scale * mods[0:1, :] + mods[1:2, :]).astype(BF16)

    def hidden(i):
        lo, n = spans[i]
        hbuf[i % 2, 0:n, :] = modulate(lat[lo:lo + n, :], wide(inv[lo:lo + n, :], d))

    hidden(0)
    for i, (lo, n) in enumerate(spans):
        r = dot(hbuf[i % 2, 0:n, :], wqkv[...])
        kv[lo + up_n:lo + up_n + n, :] = r[:, :2 * width].astype(BF16)
        q[lo:lo + n, :] = (r[:, 2 * width:] * q_scale).astype(BF16)
        if i + 1 < len(spans):
            hidden(i + 1)
        if i == 0:
            send_halo(0)
            raw_along(0)
        if i == 1:
            beside()
            send_halo(1)

    half_t = nt // 2
    my_half = tp // half_t
    base_row = sp * rows
    ones = jnp.ones((1, HEAD_DIM), BF16)

    def with_ones(v):
        return jnp.concatenate([v, jnp.broadcast_to(ones, v.shape)], axis=1)

    def window(r):
        grid_row = base_row + r
        s0 = jnp.clip(grid_row - WIN_ROWS // 2, 0, total_rows - WIN_ROWS)
        s1 = jnp.clip(grid_row + 1 - WIN_ROWS // 2, 0, total_rows - WIN_ROWS)
        win = pl.ds(pl.multiple_of((s0 - base_row + UP_ROWS) * GRID_W, GRID_W), KEYS)
        return grid_row, s0, s1, win

    def near_scores(r, h):
        grid_row, s0, s1, win = window(r)
        i0 = s0 - grid_row + WIN_ROWS - 1
        i1 = i0 - 1
        moved = s1 > s0
        lo = h * HEAD_DIM
        t = r * GRID_W
        s = dot_t(q[t:t + PAIR, lo:lo + HEAD_DIM], kv[win, lo:lo + HEAD_DIM])
        b0 = [bias[h, i0 + 2 * k] for k in range(WIN_ROWS // 2)]
        ids = [jnp.where(moved, TABLES, i1)]
        ids += [jnp.where(moved, i1 + 2 * k, i1 + 2 * k) for k in range(1, WIN_ROWS // 2)]
        ids += [jnp.where(moved, TABLES + 1, TABLES + 2)]
        b1 = [bias[h, i] for i in ids]
        x0 = s[:GRID_W, :WIN_ROWS * GRID_W] + jnp.concatenate(b0, axis=1)
        x1 = s[GRID_W:, :] + jnp.concatenate(b1, axis=1)
        s_near[h, t:t + GRID_W, 0:WIN_ROWS * GRID_W] = x0
        s_near[h, t + GRID_W:t + PAIR, :] = x1
        m = jnp.concatenate([jnp.max(x0, axis=-1, keepdims=True), jnp.max(x1, axis=-1, keepdims=True)], axis=0)
        return jnp.broadcast_to(m, (PAIR, HEAD_DIM))

    def near_values(r, h, m):
        win = window(r)[3]
        lo = h * HEAD_DIM
        t = r * GRID_W
        old = mx[h, t:t + PAIR, :]
        m = jnp.maximum(m, old)
        w = jnp.exp2(old - m)
        n0 = WIN_ROWS * GRID_W
        e0 = jnp.exp2(s_near[h, t:t + GRID_W, 0:n0] - wide(m[:GRID_W], n0)).astype(BF16)
        e1 = jnp.exp2(s_near[h, t + GRID_W:t + PAIR, :] - wide(m[GRID_W:], KEYS)).astype(BF16)
        e0 = jnp.concatenate([e0, jnp.zeros((GRID_W, KEYS - n0), BF16)], axis=1)
        p = jnp.concatenate([e0, e1], axis=0)
        o = dot(p, with_ones(kv[win, width + lo:width + lo + HEAD_DIM]))
        mx[h, t:t + PAIR, :] = m
        acc[h, t:t + PAIR, :] = acc[h, t:t + PAIR, :] * wide(w, 2 * HEAD_DIM) + o

    def near(pairs):
        units = [(r, h) for r in pairs for h in range(heads)]
        ms = [near_scores(r, h) for r, h in units]
        for (r, h), m in zip(units, ms):
            near_values(r, h, m)

    def flat(x):
        n = x.shape[0] * c_here
        if c_here % 16:
            return x.astype(F32).reshape(n, HEAD_DIM).astype(BF16)
        return x.reshape(n, HEAD_DIM)

    def far_scores(t, col, zs, h):
        lo = h * HEAD_DIM
        s = dot_t(q[t, lo:lo + HEAD_DIM], flat(ctx_all[col, zs, :, lo:lo + HEAD_DIM]))
        s_far[h, t, 0:s.shape[1]] = s
        return jnp.broadcast_to(jnp.max(s, axis=-1, keepdims=True), (own_n, HEAD_DIM))

    def far_values(t, col, zs, h, m, last):
        lo = width + h * HEAD_DIM
        v = flat(ctx_all[col, zs, :, lo:lo + HEAD_DIM])
        old = mx[h, t, :]
        m = jnp.maximum(m, old)
        w = jnp.exp2(old - m)
        n = v.shape[0]
        e = jnp.exp2(s_far[h, t, 0:n] - wide(m, n)).astype(BF16)
        o = acc[h, t, :] * wide(w, 2 * HEAD_DIM) + dot(e, with_ones(v))
        if last:
            lo = h * HEAD_DIM
            att[t, lo:lo + HEAD_DIM] = (o[:, :HEAD_DIM] / o[:, HEAD_DIM:]).astype(BF16)
        else:
            mx[h, t, :] = m
            acc[h, t, :] = o

    def far(parts, o, zs, last):
        col = (yi + o) % ny
        units = [(pl.ds(pl.multiple_of(p * own_n, 16), own_n), h) for p in parts for h in range(heads)]
        ms = [far_scores(t, col, zs, h) for t, h in units]
        for (t, h), m in zip(units, ms):
            far_values(t, col, zs, h, m, last)

    everything = pl.ds(0, nz)

    relay(1, pass_first)
    for i in range(1, RAW_PARTS):
        raw_along(i)
    near(range(UP_ROWS, rows - UP_ROWS, 2))
    relay(1, pass_second)
    send_halo(2)
    up_pairs, down_pairs = range(0, UP_ROWS, 2), range(rows - UP_ROWS, rows, 2)
    pl.when(sp == 0)(lambda: near(up_pairs))
    if nz > 2:
        relay(2, pass_first)
    send_halo(3)
    for i in range(RAW_PARTS):
        raw_over(i)
    if nz > 2:
        relay(2, pass_second)
    send_halo(4)
    for i in range(RAW_PARTS):
        raw_done(i)
    hbuf[0, 0:down_n, :] = modulate(raw[...], inv_of(raw[...]))
    below = dot(hbuf[0, 0:down_n, :], wqkv[:, 0:2 * width])
    kv[up_n + tokens:up_n + tokens + down_n, :] = below.astype(BF16)

    def halo_near():
        for i in range(len(HALO)):
            halo(i).wait_recv()
        near(up_pairs)

    if nz > 3:
        relay_down(3, pass_first)
    pl.when(my_half == 0)(lambda: near(down_pairs))
    if nz > 3:
        relay_up(3, pass_first)
    if nz > 3:
        relay(3, pass_second)

    def late_relay(k, _):
        relay(k, pass_first)
        relay(k, pass_second)
        return 0

    lax.fori_loop(4, nz, late_relay, 0)
    theirs = [(1 - my_half) * half_t + j for j in range(half_t)]
    ours = [my_half * half_t + (tp + o) % half_t for o in range(half_t)]
    low = zi < nz - nz // 2
    z_last = jnp.where(low, nz - 1, 0)
    z_rest = pl.ds(jnp.where(low, 0, 1), nz - 1)

    def others(zb):
        def other(o, _):
            arrived(0, zb * ny + (yi + o) % ny)
            return 0

        lax.fori_loop(1, ny, other, 0)

    def middle(parts, zs):
        lax.fori_loop(1, ny - 1, lambda o, c: (far(parts, o, zs, False), c)[1], 0)

    def far_own(parts):
        if ny > 1:
            far(parts, 0, everything, False)

    def far_rest(parts):
        if nz > 1:
            middle(parts, z_rest)
            far(parts, ny - 1, z_rest, False)

    far_own(theirs)
    for k in range(nz - 1):
        others(z_rest.start + k)
    far_rest(theirs)
    pl.when((my_half == 1) & has_prev)(halo_near)
    others(z_last)
    middle(theirs, pl.ds(z_last, 1))

    def settle_row(zb, _):
        pl.when(zb == zi)(lambda: across(2, zb, sent))
        pl.when(zb != zi)(lambda: across(0, zb, sent))

        @pl.when(zb <= zi)
        def _():
            upward(2, zb * ny + yi, sent)

        @pl.when(zb >= zi)
        def _():
            downward(2, zb * ny + yi, sent)

        def column(o, _):
            block = zb * ny + (yi + o) % ny

            @pl.when(zb <= zi)
            def _():
                upward(1, block, sent)

            @pl.when(zb >= zi)
            def _():
                downward(1, block, sent)

            return 0

        lax.fori_loop(1, ny, column, 0)
        return 0

    def head_copy(src, dst):
        return pltpu.make_async_remote_copy(
            src_ref=att.at[pl.ds(pl.multiple_of(dst * own_n, 16), own_n)], dst_ref=own.at[src],
            send_sem=head_s.at[(dst - src + nt - 1) % nt], recv_sem=head_r.at[(dst - src + nt - 1) % nt],
            device_id={"sp": sp, "tp": dst},
        )

    for p in theirs:
        far([p], ny - 1, pl.ds(z_last, 1), True)
        head_copy(tp, p).start()
    pl.when((my_half == 0) & has_prev)(halo_near)
    pl.when(my_half == 1)(lambda: near(down_pairs))
    far_own(ours)
    far_rest(ours)
    middle(ours, pl.ds(z_last, 1))
    far(ours[1:], ny - 1, pl.ds(z_last, 1), True)
    for p in ours[1:]:
        head_copy(tp, p).start()
    far(ours[:1], ny - 1, pl.ds(z_last, 1), True)
    for i in range(len(HALO)):
        pl.when(has_next)(lambda c=halo(i): c.wait_send())
    lax.fori_loop(0, nz, settle_row, 0)

    def wait_gate(o, _):
        tp_copy(gater, gate_s, gate_r, o).wait()
        return 0

    lax.fori_loop(1, nt, wait_gate, 0)
    gsum = gater[0]
    for i in range(1, nt):
        gsum = gsum + gater[i]
    gates[...] = jnp.concatenate([gsum[j:j + 1] for j in range(8)], axis=1)
    wo_load.wait()
    own_load.wait()

    def part_of(p):
        return pl.ds(pl.multiple_of(p * width, HEAD_DIM), width)

    for n0 in range(0, d, step):
        y_own[:, n0:n0 + step] = dot(att[my_rows, :], wo[part_of(tp), n0:n0 + step])
    for p in ours[1:]:
        head_copy(p, tp).wait_recv()
        for n0 in range(0, d, step):
            y_own[:, n0:n0 + step] += dot(own[p], wo[part_of(p), n0:n0 + step])
    for p in theirs:
        head_copy(p, tp).wait_recv()
    for p in theirs + ours[1:]:
        head_copy(tp, p).wait_send()


def finish(own, wo, gates, lat_own, y_own, out, buf, sem):
    nt, _, width = own.shape
    d = wo.shape[1]
    step = d // 4
    half_t = nt // 2
    other = (1 - lax.axis_index("tp") // half_t) * half_t
    a = jnp.concatenate([own[other + i] for i in range(half_t)], axis=1)
    rows = pl.ds(pl.multiple_of(other * width, HEAD_DIM), half_t * width)
    copies = []
    for i in range(4):
        cols = pl.ds(i * step, step)
        y = y_own[:, cols] + dot(a, wo[rows, cols])
        buf[:, cols] = (lat_own[:, cols].astype(F32) + gates[:, cols] * y).astype(BF16)
        copies.append(pltpu.make_async_copy(buf.at[:, cols], out.at[:, cols], sem.at[i]))
        copies[-1].start()
    for c in copies:
        c.wait()


def shards(
    ns, nt,
    latents, cond, ctx_cond, context, norm_gain, shift_weight, scale_weight, gate_weight,
    q_weight, k_weight, v_weight, out_weight, rel_bias,
):
    tokens, d = latents.shape
    c_here = context.shape[0]
    kt = shift_weight.shape[0]
    width = q_weight.shape[1]
    heads = width // HEAD_DIM
    own_n = tokens // nt
    table = jnp.transpose(rel_bias, (1, 0, 2))
    ny = 1
    while ns % (2 * ny) == 0 and 4 * ny * ny <= ns:
        ny *= 2
    halo = (UP_ROWS + DOWN_ROWS + 1) * GRID_W
    vmem = pl.BlockSpec(memory_space=pltpu.VMEM)
    hbm = pl.BlockSpec(memory_space=pltpu.HBM)
    sem = pltpu.SemaphoreType.DMA
    tail = 8 * 1024 * 1024
    parts = pl.pallas_call(
        functools.partial(kernel, ns, nt, ny),
        out_shape=(
            pltpu.VMEM((nt, own_n, width), BF16),
            pltpu.VMEM(out_weight.shape, BF16),
            pltpu.VMEM((1, d), F32),
            pltpu.VMEM((own_n, d), BF16),
            pltpu.VMEM((own_n, d), F32),
        ),
        in_specs=[hbm] * 13,
        out_specs=(vmem,) * 5,
        scratch_shapes=[
            pltpu.VMEM((tokens, d), BF16),
            pltpu.VMEM((c_here, d), BF16),
            pltpu.VMEM((kt, d), BF16),
            pltpu.VMEM((kt, d), BF16),
            pltpu.VMEM((kt, d), BF16),
            pltpu.VMEM((d, 3 * width), BF16),
            pltpu.VMEM((d // 2 // 512, nt, 8, 512), F32),
            pltpu.VMEM((nt, 8, d // 8), F32),
            pltpu.VMEM((8, d), F32),
            pltpu.VMEM((tokens, HEAD_DIM), F32),
            pltpu.VMEM((2, UP_ROWS * GRID_W, d), BF16),
            pltpu.VMEM((ny, ns // ny, c_here, 2 * width), BF16),
            pltpu.VMEM((tokens + halo, 2 * width), BF16),
            pltpu.VMEM((tokens, width), BF16),
            pltpu.VMEM((DOWN_ROWS * GRID_W, d), BF16),
            pltpu.VMEM((heads, TABLES + 3, GRID_W, PAIR), F32),
            pltpu.VMEM((heads, tokens, KEYS), F32),
            pltpu.VMEM((heads, tokens, ns // ny * c_here), F32),
            pltpu.VMEM((heads, tokens, 2 * HEAD_DIM), F32),
            pltpu.VMEM((heads, tokens, HEAD_DIM), F32),
            pltpu.VMEM((tokens, width), BF16),
            pltpu.VMEM((2 * WIN_ROWS - 1, heads, PAIR), F32),
            pltpu.VMEM((1, d), F32),
            pltpu.VMEM((1, d), F32),
            pltpu.VMEM((1, d), F32),
            pltpu.VMEM(table.shape, F32),
            sem((12 + d // 2 // 512,)),
            sem((nt - 1,)), sem((nt - 1,)), sem((nt - 1,)), sem((nt - 1,)),
            sem((ns // ny, max(ny - 1, 1))), sem((2, ns)), sem((2, ns)),
            sem((len(HALO),)), sem((len(HALO),)),
            sem((RAW_PARTS, 2 * (nt // CORES))), sem((RAW_PARTS, nt)),
            sem((nt - 1,)), sem((nt - 1,)),
        ],
        compiler_params=pltpu.CompilerParams(
            collective_id=0, has_side_effects=True, vmem_limit_bytes=VMEM_BYTES - tail
        ),
    )(
        cond[None], ctx_cond[None], norm_gain[None], table, latents, context, shift_weight, scale_weight, gate_weight,
        q_weight, k_weight, v_weight, out_weight,
    )
    return pl.pallas_call(
        finish,
        out_shape=jax.ShapeDtypeStruct((own_n, d), BF16),
        in_specs=[vmem] * 5,
        out_specs=hbm,
        scratch_shapes=[pltpu.VMEM((own_n, d), BF16), sem((4,))],
        compiler_params=pltpu.CompilerParams(vmem_limit_bytes=16 * 1024 * 1024),
    )(*parts)


def solution(mesh):
    in_specs = (
        P("sp", None),
        P(),
        P(),
        P("sp", None),
        P(),
        P("tp", None),
        P("tp", None),
        P("tp", None),
        P(None, "tp"),
        P(None, "tp"),
        P(None, "tp"),
        P(),
        P("tp", None, None),
    )
    body = functools.partial(shards, mesh.shape["sp"], mesh.shape["tp"])
    return jax.shard_map(
        body, mesh=mesh, in_specs=in_specs, out_specs=P(("sp", "tp"), None), check_vma=False
    )
```

```python
import functools

import jax
import jax.numpy as jnp
from jax import lax
from jax.experimental import pallas as pl
from jax.experimental.pallas import tpu as pltpu
from jax.sharding import PartitionSpec as P

HEAD_DIM = 128
GRID_W = 64
WIN_ROWS = 8
WIN_COLS = 16
EPS = 1e-06
NEG_BIG = -1e30
F32 = jnp.float32
BF16 = jnp.bfloat16
UP_ROWS = WIN_ROWS // 2
DOWN_ROWS = WIN_ROWS // 2 - 1
PAIR = 2 * GRID_W
KEY_ROWS = WIN_ROWS + 2
KEYS = KEY_ROWS * GRID_W
TABLES = 2 * WIN_ROWS - 2
Z_FIRST = 3
HALO = ((0, 2), (2, 2))
ISSUE = ((), ((0, 0), (1, 2)), (), (), ((1, 1),))
RAW_PARTS = 1
CORES = 2
VMEM_BYTES = 67043328


def dot(a, b):
    return jnp.dot(a, b, preferred_element_type=F32)


def dot_t(a, b):
    return lax.dot_general(a, b, (((1,), (1,)), ((), ())), preferred_element_type=F32)


def wide(x, n):
    return jnp.concatenate([x] * pl.cdiv(n, HEAD_DIM), axis=1)[:, :n]


def kernel(
    ns, nt, ny,
    cond_h, ctx_cond_h, gain_h, table_h,
    lat_h, ctx_h, wsh_h, wsc_h, wg_h, wq_h, wk_h, wv_h, wo_h,
    own, wo, gates, lat_own, y_own,
    lat, ctx, wsh, wsc, wg, wqkv,
    modr, gater, mods, inv, hbuf, ctx_all, kv, q, raw, bias, s_near, s_far, acc, mx, att, lines,
    cond, ctx_cond, gain, table,
    load_sem, mod_s, mod_r, gate_s, gate_r, across_s, along_s, ctx_r, halo_s, halo_r, raw_s, raw_r, head_s, head_r,
):
    sp, tp = lax.axis_index("sp"), lax.axis_index("tp")
    tokens, d = lat.shape
    c_here = ctx.shape[0]
    width = q.shape[1]
    heads = width // HEAD_DIM
    kt = wsh.shape[0]
    rows = tokens // GRID_W
    total_rows = rows * ns
    own_n = tokens // nt
    up_n, down_n = UP_ROWS * GRID_W, DOWN_ROWS * GRID_W
    to_log2 = 1.4426950408889634
    q_scale = HEAD_DIM ** -0.5 * to_log2
    half_d = d // 2
    step = 512

    count = [0]

    def load(s, t, same=None):
        if same is None:
            same = count[0]
            count[0] += 1
        return pltpu.make_async_copy(s, t, load_sem.at[same])

    small = [load(cond_h, cond), load(ctx_cond_h, ctx_cond), load(gain_h, gain), load(table_h, table)]
    mod_loads, mod_slots = [], []
    for n0 in range(0, half_d, step):
        slot_here = count[0]
        mod_slots.append(slot_here)
        count[0] += 1
        mod_loads.append([
            load(s.at[:, pl.ds(k * half_d + n0, step)], t.at[:, pl.ds(k * half_d + n0, step)], slot_here)
            for k in range(2) for s, t in ((wsh_h, wsh), (wsc_h, wsc))
        ])
    ctx_load, lat_load, wg_load = load(ctx_h, ctx), load(lat_h, lat), load(wg_h, wg)
    wk_load = load(wk_h, wqkv.at[:, pl.ds(0, width)])
    wv_load = load(wv_h, wqkv.at[:, pl.ds(width, width)])
    wq_load = load(wq_h, wqkv.at[:, pl.ds(2 * width, width)])
    wo_load = load(wo_h, wo)
    my_rows = pl.ds(pl.multiple_of(tp * own_n, 16), own_n)
    own_load = load(lat_h.at[my_rows], lat_own)
    for c in small + sum(mod_loads, []) + [ctx_load, lat_load]:
        c.start()

    barrier = pltpu.get_barrier_semaphore()

    def greet_tp(o, _):
        pl.semaphore_signal(barrier, inc=1, device_id={"sp": sp, "tp": (tp + o) % nt})
        return 0

    def greet_sp(o, _):
        pl.semaphore_signal(barrier, inc=1, device_id={"sp": (sp + o) % ns, "tp": tp})
        return 0

    lax.fori_loop(1, nt, greet_tp, 0)
    lax.fori_loop(1, ns, greet_sp, 0)

    for c in small:
        c.wait()

    start = pl.multiple_of(tp * kt, 128)
    row = lax.broadcasted_iota(jnp.int32, (8, kt), 0)

    def silu(ref):
        v = ref[:, pl.ds(start, kt)]
        return jnp.broadcast_to(v / (1.0 + jnp.exp(-v)), (8, kt))

    row0_act = silu(cond)
    mixed_act = jnp.where(row % 2 == 0, row0_act, silu(ctx_cond))

    def only(a, keep):
        return jnp.where(keep, a, 0.0).astype(BF16)

    a_sh = [only(mixed_act, (row // 2) == 2 * k) for k in range(2)]
    a_sc = [only(mixed_act, (row // 2) == 2 * k + 1) for k in range(2)]
    def mod_copy(i, o):
        return pltpu.make_async_remote_copy(
            src_ref=modr.at[i, tp], dst_ref=modr.at[i, tp],
            send_sem=mod_s.at[o - 1], recv_sem=mod_r.at[o - 1],
            device_id={"sp": sp, "tp": (tp + o) % nt},
        )

    def each_mod(i, act):
        def one(o, _):
            act(mod_copy(i, o))
            return 0

        lax.fori_loop(1, nt, one, 0)

    chunks = half_d // step
    for i in range(chunks):
        load(wsh_h.at[:, pl.ds(0, 4 * step)], wsh.at[:, pl.ds(0, 4 * step)], mod_slots[i]).wait()
        part = jnp.zeros((8, step), F32)
        for k in range(2):
            cols = pl.ds(k * half_d + i * step, step)
            part = part + dot(a_sh[k], wsh[:, cols])
            part = part + dot(a_sc[k], wsc[:, cols])
        modr[i, tp] = part
        if i == 0:
            pl.semaphore_wait(barrier, nt - 1 + ns - 1)
        each_mod(i, lambda c: c.start())
    quarter = down_n // nt
    piece = quarter // RAW_PARTS
    nx = nt // CORES
    core, xi = tp % CORES, tp // CORES
    has_next, has_prev = sp < ns - 1, sp > 0

    def raw_at(i, t):
        return raw.at[pl.ds(pl.multiple_of(t * quarter, 8) + i * piece, piece)]

    def raw_first(i):
        src = lat_h.at[pl.ds(pl.multiple_of(tp * quarter, 8) + i * piece, piece)]
        return pltpu.make_async_remote_copy(
            src_ref=src, dst_ref=raw_at(i, tp), send_sem=raw_s.at[i, 0], recv_sem=raw_r.at[i, tp],
            device_id={"sp": (sp + ns - 1) % ns, "tp": tp},
        )

    def raw_next(i, t, dest, lane):
        return pltpu.make_async_remote_copy(
            src_ref=raw_at(i, t), dst_ref=raw_at(i, t), send_sem=raw_s.at[i, lane], recv_sem=raw_r.at[i, t],
            device_id={"sp": sp, "tp": dest},
        )

    def raw_x(i, o):
        return raw_next(i, tp, (xi + o) % nx * CORES + core, o)

    def raw_mate(i, o):
        return raw_next(i, (xi + o) % nx * CORES + core, xi * CORES + (core + 1) % CORES, nx + o)

    def raw_got(i, t):
        raw_next(i, t, tp, 0).wait_recv()

    def raw_along(i):
        @pl.when(has_next)
        def _():
            raw_got(i, tp)
            for o in range(1, nx):
                raw_x(i, o).start()
            raw_mate(i, 0).start()

    def raw_over(i):
        @pl.when(has_next)
        def _():
            for o in range(1, nx):
                raw_got(i, (xi + o) % nx * CORES + core)
                raw_mate(i, o).start()

    def raw_done(i):
        @pl.when(has_prev)
        def _():
            raw_first(i).wait_send()

        @pl.when(has_next)
        def _():
            for o in range(nx):
                raw_got(i, (xi + o) % nx * CORES + (core + 1) % CORES)
                raw_mate(i, o).wait_send()
                if o:
                    raw_x(i, o).wait_send()

    @pl.when(has_prev)
    def _():
        for i in range(RAW_PARTS):
            raw_first(i).start()

    for c in [wg_load, wk_load, wv_load, wq_load, wo_load, own_load]:
        c.start()

    def tp_copy(buf, s_sem, r_sem, o):
        return pltpu.make_async_remote_copy(
            src_ref=buf.at[tp], dst_ref=buf.at[tp],
            send_sem=s_sem.at[o - 1], recv_sem=r_sem.at[o - 1],
            device_id={"sp": sp, "tp": (tp + o) % nt},
        )

    qc = lax.broadcasted_iota(jnp.int32, (GRID_W, PAIR), 0)
    lane = lax.broadcasted_iota(jnp.int32, (GRID_W, PAIR), 1)
    kc = lane % GRID_W
    first = jnp.clip(qc - WIN_COLS // 2, 0, GRID_W - WIN_COLS)
    inside = (kc >= first) & (kc < first + WIN_COLS)
    lines[...] = jnp.zeros_like(lines)
    lines[:, :, 0:2 * WIN_COLS - 1] = table[...]
    low_row = WIN_ROWS - 1 - WIN_ROWS // 2
    for h in range(heads):
        for i in range(TABLES):
            near_line = jnp.broadcast_to(lines[i, h:h + 1, :], (GRID_W, PAIR))
            next_line = jnp.broadcast_to(lines[i + 1, h:h + 1, :], (GRID_W, PAIR))
            reach = WIN_COLS - 1
            rolled = pltpu.roll(near_line, PAIR - reach, 1, stride=1, stride_axis=0)
            rolled = rolled + pltpu.roll(next_line, GRID_W - reach, 1, stride=1, stride_axis=0)
            both = jnp.where(inside, rolled * to_log2, NEG_BIG)
            bias[h, i] = both
            if i == low_row - 1:
                bias[h, TABLES] = jnp.where(lane >= GRID_W, both, NEG_BIG)
            if i == low_row + WIN_ROWS - 1:
                bias[h, TABLES + 1] = jnp.where(lane < GRID_W, both, NEG_BIG)
        bias[h, TABLES + 2] = jnp.full((GRID_W, PAIR), NEG_BIG, F32)
    mx[...] = jnp.full_like(mx, NEG_BIG)
    acc[...] = jnp.zeros_like(acc)
    n_keys = kv.shape[0] - tokens - up_n

    @pl.when(sp == ns - 1)
    def _():
        raw[...] = jnp.zeros_like(raw)

    @pl.when(sp == 0)
    def _():
        kv[0:up_n, :] = jnp.zeros((up_n, 2 * width), BF16)

    kv[pl.ds(up_n + tokens + down_n, n_keys - down_n), :] = jnp.zeros((n_keys - down_n, 2 * width), BF16)

    def inv_of(x):
        xf = x.astype(F32)
        return lax.rsqrt(jnp.mean(xf * xf, axis=-1, keepdims=True) + EPS)

    ctx_load.wait()
    ctx_inv = inv_of(ctx[...])
    lat_load.wait()
    for t in range(0, tokens, GRID_W):
        inv[t:t + GRID_W, :] = jnp.broadcast_to(inv_of(lat[t:t + GRID_W, :]), (GRID_W, HEAD_DIM))

    wg_load.wait()
    seg = d // 8
    gp = jnp.zeros((8, seg), F32)
    for j in range(8):
        gp = gp + dot(only(row0_act, row == j), wg[:, pl.ds(j * seg, seg)])
    gater[tp] = gp

    def start_gate(o, _):
        tp_copy(gater, gate_s, gate_r, o).start()
        return 0

    lax.fori_loop(1, nt, start_gate, 0)
    wk_load.wait()
    wv_load.wait()

    each_mod(pl.ds(0, chunks), lambda c: c.wait())
    g = gain[...]
    for i in range(chunks):
        total = modr[i, 0]
        for j in range(1, nt):
            total = total + modr[i, j]
        for k in range(2):
            lo = k * half_d + i * step
            cols = pl.ds(lo, step)
            gk = g[:, lo:lo + step]
            mods[0:1, cols] = gk * (1.0 + total[4 * k + 2:4 * k + 3])
            mods[1:2, cols] = total[4 * k:4 * k + 1]
            mods[2:3, cols] = gk * (1.0 + total[4 * k + 3:4 * k + 4])
            mods[3:4, cols] = total[4 * k + 1:4 * k + 2]

    ctx_hid = (ctx[...].astype(F32) * ctx_inv * mods[2:3, :] + mods[3:4, :]).astype(BF16)
    ctx_all[sp % ny, sp // ny] = dot(ctx_hid, wqkv[:, 0:2 * width]).astype(BF16)

    nz = ns // ny
    zi, yi = sp // ny, sp % ny

    cut = max(Z_FIRST * width // 2 // HEAD_DIM, 1) * HEAD_DIM

    def ctx_copy(part, block, dest, send_sem):
        cols = (pl.ds(0, cut), pl.ds(cut, 2 * width - cut), pl.ds(0, 2 * width))[part]
        ref = ctx_all.at[block % ny, block // ny, :, cols]
        return pltpu.make_async_remote_copy(
            src_ref=ref, dst_ref=ref, send_sem=send_sem, recv_sem=ctx_r.at[part % 2, block],
            device_id={"sp": dest, "tp": tp},
        )

    def across(part, zb, act):
        def one(o, _):
            act(ctx_copy(part, zb * ny + yi, zi * ny + (yi + o) % ny, across_s.at[zb, o - 1]))
            return 0

        lax.fori_loop(1, ny, one, 0)

    def upward(part, block, act):
        @pl.when(zi < nz - 1)
        def _():
            act(ctx_copy(part, block, sp + ny, along_s.at[0, block]))

    def downward(part, block, act):
        @pl.when(zi > 0)
        def _():
            act(ctx_copy(part, block, sp - ny, along_s.at[1, block]))

    def go(c):
        c.start()

    def sent(c):
        c.wait_send()

    def arrived(part, block):
        ctx_copy(part, block, sp, along_s.at[0, block]).wait_recv()

    def beside():
        def one(o, _):
            block = zi * ny + (yi + o) % ny
            arrived(1, block)
            upward(1, block, go)
            downward(1, block, go)
            return 0

        lax.fori_loop(1, ny, one, 0)

    def pass_first(zb, forward):
        block = zb * ny + yi
        arrived(0, block)
        forward(0, block, go)
        across(0, zb, go)

    def pass_second(zb, forward):
        def one(o, _):
            other = zb * ny + (yi + o) % ny
            arrived(1, other)
            forward(1, other, go)
            return 0

        lax.fori_loop(0, ny, one, 0)

    def relay_down(k, pass_on):
        @pl.when(zi + k < nz)
        def _():
            pass_on(zi + k, downward)

    def relay_up(k, pass_on):
        @pl.when(zi - k >= 0)
        def _():
            pass_on(zi - k, upward)

    def relay(k, pass_on):
        relay_down(k, pass_on)
        relay_up(k, pass_on)

    across(1, zi, go)
    for part in range(2):
        upward(part, sp, go)
        downward(part, sp, go)
    across(0, zi, go)

    def halo(i):
        lo, n = HALO[i]
        return pltpu.make_async_remote_copy(
            src_ref=kv.at[pl.ds(tokens + lo * GRID_W, n * GRID_W)],
            dst_ref=kv.at[pl.ds(lo * GRID_W, n * GRID_W)],
            send_sem=halo_s.at[i], recv_sem=halo_r.at[i],
            device_id={"sp": (sp + 1) % ns, "tp": tp},
        )

    def send_halo(point):
        for i, which in ISSUE[point]:
            turn = (yi >= 0, yi == ny - 1, yi < ny - 1)[which]
            pl.when(has_next & turn)(lambda c=halo(i): c.start())

    wq_load.wait()
    rest = (tokens - up_n) // 2
    spans = [(tokens - up_n, up_n), (0, rest), (rest, rest)]

    def modulate(x, scale):
        return (x.astype(F32) * scale * mods[0:1, :] + mods[1:2, :]).astype(BF16)

    def hidden(i):
        lo, n = spans[i]
        hbuf[i % 2, 0:n, :] = modulate(lat[lo:lo + n, :], wide(inv[lo:lo + n, :], d))

    hidden(0)
    for i, (lo, n) in enumerate(spans):
        r = dot(hbuf[i % 2, 0:n, :], wqkv[...])
        kv[lo + up_n:lo + up_n + n, :] = r[:, :2 * width].astype(BF16)
        q[lo:lo + n, :] = (r[:, 2 * width:] * q_scale).astype(BF16)
        if i + 1 < len(spans):
            hidden(i + 1)
        if i == 0:
            send_halo(0)
            raw_along(0)
        if i == 1:
            beside()
            send_halo(1)

    half_t = nt // 2
    my_half = tp // half_t
    base_row = sp * rows
    ones = jnp.ones((1, HEAD_DIM), BF16)

    def with_ones(v):
        return jnp.concatenate([v, jnp.broadcast_to(ones, v.shape)], axis=1)

    def window(r):
        grid_row = base_row + r
        s0 = jnp.clip(grid_row - WIN_ROWS // 2, 0, total_rows - WIN_ROWS)
        s1 = jnp.clip(grid_row + 1 - WIN_ROWS // 2, 0, total_rows - WIN_ROWS)
        win = pl.ds(pl.multiple_of((s0 - base_row + UP_ROWS) * GRID_W, GRID_W), KEYS)
        return grid_row, s0, s1, win

    def near_scores(r, h):
        grid_row, s0, s1, win = window(r)
        i0 = s0 - grid_row + WIN_ROWS - 1
        i1 = i0 - 1
        moved = s1 > s0
        lo = h * HEAD_DIM
        t = r * GRID_W
        s = dot_t(q[t:t + PAIR, lo:lo + HEAD_DIM], kv[win, lo:lo + HEAD_DIM])
        b0 = [bias[h, i0 + 2 * k] for k in range(WIN_ROWS // 2)]
        ids = [jnp.where(moved, TABLES, i1)]
        ids += [jnp.where(moved, i1 + 2 * k, i1 + 2 * k) for k in range(1, WIN_ROWS // 2)]
        ids += [jnp.where(moved, TABLES + 1, TABLES + 2)]
        b1 = [bias[h, i] for i in ids]
        x0 = s[:GRID_W, :WIN_ROWS * GRID_W] + jnp.concatenate(b0, axis=1)
        x1 = s[GRID_W:, :] + jnp.concatenate(b1, axis=1)
        s_near[h, t:t + GRID_W, 0:WIN_ROWS * GRID_W] = x0
        s_near[h, t + GRID_W:t + PAIR, :] = x1
        m = jnp.concatenate([jnp.max(x0, axis=-1, keepdims=True), jnp.max(x1, axis=-1, keepdims=True)], axis=0)
        return jnp.broadcast_to(m, (PAIR, HEAD_DIM))

    def near_values(r, h, m):
        win = window(r)[3]
        lo = h * HEAD_DIM
        t = r * GRID_W
        old = mx[h, t:t + PAIR, :]
        m = jnp.maximum(m, old)
        w = jnp.exp2(old - m)
        n0 = WIN_ROWS * GRID_W
        e0 = jnp.exp2(s_near[h, t:t + GRID_W, 0:n0] - wide(m[:GRID_W], n0)).astype(BF16)
        e1 = jnp.exp2(s_near[h, t + GRID_W:t + PAIR, :] - wide(m[GRID_W:], KEYS)).astype(BF16)
        e0 = jnp.concatenate([e0, jnp.zeros((GRID_W, KEYS - n0), BF16)], axis=1)
        p = jnp.concatenate([e0, e1], axis=0)
        o = dot(p, with_ones(kv[win, width + lo:width + lo + HEAD_DIM]))
        mx[h, t:t + PAIR, :] = m
        acc[h, t:t + PAIR, :] = acc[h, t:t + PAIR, :] * wide(w, 2 * HEAD_DIM) + o

    def near(pairs):
        units = [(r, h) for r in pairs for h in range(heads)]
        ms = [near_scores(r, h) for r, h in units]
        for (r, h), m in zip(units, ms):
            near_values(r, h, m)

    def flat(x):
        n = x.shape[0] * c_here
        if c_here % 16:
            return x.astype(F32).reshape(n, HEAD_DIM).astype(BF16)
        return x.reshape(n, HEAD_DIM)

    def far_scores(t, col, zs, h):
        lo = h * HEAD_DIM
        s = dot_t(q[t, lo:lo + HEAD_DIM], flat(ctx_all[col, zs, :, lo:lo + HEAD_DIM]))
        s_far[h, t, 0:s.shape[1]] = s
        return jnp.broadcast_to(jnp.max(s, axis=-1, keepdims=True), (own_n, HEAD_DIM))

    def far_values(t, col, zs, h, m, last):
        lo = width + h * HEAD_DIM
        v = flat(ctx_all[col, zs, :, lo:lo + HEAD_DIM])
        old = mx[h, t, :]
        m = jnp.maximum(m, old)
        w = jnp.exp2(old - m)
        n = v.shape[0]
        e = jnp.exp2(s_far[h, t, 0:n] - wide(m, n)).astype(BF16)
        o = acc[h, t, :] * wide(w, 2 * HEAD_DIM) + dot(e, with_ones(v))
        if last:
            lo = h * HEAD_DIM
            att[t, lo:lo + HEAD_DIM] = (o[:, :HEAD_DIM] / o[:, HEAD_DIM:]).astype(BF16)
        else:
            mx[h, t, :] = m
            acc[h, t, :] = o

    def far(parts, o, zs, last):
        col = (yi + o) % ny
        units = [(pl.ds(pl.multiple_of(p * own_n, 16), own_n), h) for p in parts for h in range(heads)]
        ms = [far_scores(t, col, zs, h) for t, h in units]
        for (t, h), m in zip(units, ms):
            far_values(t, col, zs, h, m, last)

    everything = pl.ds(0, nz)

    relay(1, pass_first)
    for i in range(1, RAW_PARTS):
        raw_along(i)
    near(range(UP_ROWS, rows - UP_ROWS, 2))
    relay(1, pass_second)
    send_halo(2)
    up_pairs, down_pairs = range(0, UP_ROWS, 2), range(rows - UP_ROWS, rows, 2)
    pl.when(sp == 0)(lambda: near(up_pairs))
    if nz > 2:
        relay(2, pass_first)
    send_halo(3)
    for i in range(RAW_PARTS):
        raw_over(i)
    if nz > 2:
        relay(2, pass_second)
    send_halo(4)
    for i in range(RAW_PARTS):
        raw_done(i)
    hbuf[0, 0:down_n, :] = modulate(raw[...], inv_of(raw[...]))
    below = dot(hbuf[0, 0:down_n, :], wqkv[:, 0:2 * width])
    kv[up_n + tokens:up_n + tokens + down_n, :] = below.astype(BF16)

    def halo_near():
        for i in range(len(HALO)):
            halo(i).wait_recv()
        near(up_pairs)

    if nz > 3:
        relay_down(3, pass_first)
    pl.when(my_half == 0)(lambda: near(down_pairs))
    if nz > 3:
        relay_up(3, pass_first)
    if nz > 3:
        relay(3, pass_second)

    def late_relay(k, _):
        relay(k, pass_first)
        relay(k, pass_second)
        return 0

    lax.fori_loop(4, nz, late_relay, 0)
    theirs = [(1 - my_half) * half_t + j for j in range(half_t)]
    ours = [my_half * half_t + (tp + o) % half_t for o in range(half_t)]
    low = zi < nz - nz // 2
    z_last = jnp.where(low, nz - 1, 0)
    z_rest = pl.ds(jnp.where(low, 0, 1), nz - 1)

    def others(zb):
        def other(o, _):
            arrived(0, zb * ny + (yi + o) % ny)
            return 0

        lax.fori_loop(1, ny, other, 0)

    def middle(parts, zs):
        lax.fori_loop(1, ny - 1, lambda o, c: (far(parts, o, zs, False), c)[1], 0)

    def far_own(parts):
        if ny > 1:
            far(parts, 0, everything, False)

    def far_rest(parts):
        if nz > 1:
            middle(parts, z_rest)
            far(parts, ny - 1, z_rest, False)

    far_own(theirs)
    for k in range(nz - 1):
        others(z_rest.start + k)
    far_rest(theirs)
    pl.when((my_half == 1) & has_prev)(halo_near)
    others(z_last)
    middle(theirs, pl.ds(z_last, 1))

    def settle_row(zb, _):
        pl.when(zb == zi)(lambda: across(2, zb, sent))
        pl.when(zb != zi)(lambda: across(0, zb, sent))

        @pl.when(zb <= zi)
        def _():
            upward(2, zb * ny + yi, sent)

        @pl.when(zb >= zi)
        def _():
            downward(2, zb * ny + yi, sent)

        def column(o, _):
            block = zb * ny + (yi + o) % ny

            @pl.when(zb <= zi)
            def _():
                upward(1, block, sent)

            @pl.when(zb >= zi)
            def _():
                downward(1, block, sent)

            return 0

        lax.fori_loop(1, ny, column, 0)
        return 0

    def head_copy(src, dst):
        return pltpu.make_async_remote_copy(
            src_ref=att.at[pl.ds(pl.multiple_of(dst * own_n, 16), own_n)], dst_ref=own.at[src],
            send_sem=head_s.at[(dst - src + nt - 1) % nt], recv_sem=head_r.at[(dst - src + nt - 1) % nt],
            device_id={"sp": sp, "tp": dst},
        )

    for p in theirs:
        far([p], ny - 1, pl.ds(z_last, 1), True)
        head_copy(tp, p).start()
    pl.when((my_half == 0) & has_prev)(halo_near)
    pl.when(my_half == 1)(lambda: near(down_pairs))
    far_own(ours)
    far_rest(ours)
    middle(ours, pl.ds(z_last, 1))
    far(ours[1:], ny - 1, pl.ds(z_last, 1), True)
    for p in ours[1:]:
        head_copy(tp, p).start()
    far(ours[:1], ny - 1, pl.ds(z_last, 1), True)
    for i in range(len(HALO)):
        pl.when(has_next)(lambda c=halo(i): c.wait_send())
    lax.fori_loop(0, nz, settle_row, 0)

    def wait_gate(o, _):
        tp_copy(gater, gate_s, gate_r, o).wait()
        return 0

    lax.fori_loop(1, nt, wait_gate, 0)
    gsum = gater[0]
    for i in range(1, nt):
        gsum = gsum + gater[i]
    gates[...] = jnp.concatenate([gsum[j:j + 1] for j in range(8)], axis=1)
    wo_load.wait()
    own_load.wait()

    def part_of(p):
        return pl.ds(pl.multiple_of(p * width, HEAD_DIM), width)

    for n0 in range(0, d, step):
        y_own[:, n0:n0 + step] = dot(att[my_rows, :], wo[part_of(tp), n0:n0 + step])
    for p in ours[1:]:
        head_copy(p, tp).wait_recv()
        for n0 in range(0, d, step):
            y_own[:, n0:n0 + step] += dot(own[p], wo[part_of(p), n0:n0 + step])
    for p in theirs:
        head_copy(p, tp).wait_recv()
    for p in theirs + ours[1:]:
        head_copy(tp, p).wait_send()


def finish(own, wo, gates, lat_own, y_own, out, buf, sem):
    nt, _, width = own.shape
    d = wo.shape[1]
    step = d // 4
    half_t = nt // 2
    other = (1 - lax.axis_index("tp") // half_t) * half_t
    a = jnp.concatenate([own[other + i] for i in range(half_t)], axis=1)
    rows = pl.ds(pl.multiple_of(other * width, HEAD_DIM), half_t * width)
    copies = []
    for i in range(4):
        cols = pl.ds(i * step, step)
        y = y_own[:, cols] + dot(a, wo[rows, cols])
        buf[:, cols] = (lat_own[:, cols].astype(F32) + gates[:, cols] * y).astype(BF16)
        copies.append(pltpu.make_async_copy(buf.at[:, cols], out.at[:, cols], sem.at[i]))
        copies[-1].start()
    for c in copies:
        c.wait()


def shards(
    ns, nt,
    latents, cond, ctx_cond, context, norm_gain, shift_weight, scale_weight, gate_weight,
    q_weight, k_weight, v_weight, out_weight, rel_bias,
):
    tokens, d = latents.shape
    c_here = context.shape[0]
    kt = shift_weight.shape[0]
    width = q_weight.shape[1]
    heads = width // HEAD_DIM
    own_n = tokens // nt
    table = jnp.transpose(rel_bias, (1, 0, 2))
    ny = 1
    while ns % (2 * ny) == 0 and 4 * ny * ny <= ns:
        ny *= 2
    halo = (UP_ROWS + DOWN_ROWS + 1) * GRID_W
    vmem = pl.BlockSpec(memory_space=pltpu.VMEM)
    hbm = pl.BlockSpec(memory_space=pltpu.HBM)
    sem = pltpu.SemaphoreType.DMA
    tail = 8 * 1024 * 1024
    parts = pl.pallas_call(
        functools.partial(kernel, ns, nt, ny),
        out_shape=(
            pltpu.VMEM((nt, own_n, width), BF16),
            pltpu.VMEM(out_weight.shape, BF16),
            pltpu.VMEM((1, d), F32),
            pltpu.VMEM((own_n, d), BF16),
            pltpu.VMEM((own_n, d), F32),
        ),
        in_specs=[hbm] * 13,
        out_specs=(vmem,) * 5,
        scratch_shapes=[
            pltpu.VMEM((tokens, d), BF16),
            pltpu.VMEM((c_here, d), BF16),
            pltpu.VMEM((kt, d), BF16),
            pltpu.VMEM((kt, d), BF16),
            pltpu.VMEM((kt, d), BF16),
            pltpu.VMEM((d, 3 * width), BF16),
            pltpu.VMEM((d // 2 // 512, nt, 8, 512), F32),
            pltpu.VMEM((nt, 8, d // 8), F32),
            pltpu.VMEM((8, d), F32),
            pltpu.VMEM((tokens, HEAD_DIM), F32),
            pltpu.VMEM((2, UP_ROWS * GRID_W, d), BF16),
            pltpu.VMEM((ny, ns // ny, c_here, 2 * width), BF16),
            pltpu.VMEM((tokens + halo, 2 * width), BF16),
            pltpu.VMEM((tokens, width), BF16),
            pltpu.VMEM((DOWN_ROWS * GRID_W, d), BF16),
            pltpu.VMEM((heads, TABLES + 3, GRID_W, PAIR), F32),
            pltpu.VMEM((heads, tokens, KEYS), F32),
            pltpu.VMEM((heads, tokens, ns // ny * c_here), F32),
            pltpu.VMEM((heads, tokens, 2 * HEAD_DIM), F32),
            pltpu.VMEM((heads, tokens, HEAD_DIM), F32),
            pltpu.VMEM((tokens, width), BF16),
            pltpu.VMEM((2 * WIN_ROWS - 1, heads, PAIR), F32),
            pltpu.VMEM((1, d), F32),
            pltpu.VMEM((1, d), F32),
            pltpu.VMEM((1, d), F32),
            pltpu.VMEM(table.shape, F32),
            sem((12 + d // 2 // 512,)),
            sem((nt - 1,)), sem((nt - 1,)), sem((nt - 1,)), sem((nt - 1,)),
            sem((ns // ny, max(ny - 1, 1))), sem((2, ns)), sem((2, ns)),
            sem((len(HALO),)), sem((len(HALO),)),
            sem((RAW_PARTS, 2 * (nt // CORES))), sem((RAW_PARTS, nt)),
            sem((nt - 1,)), sem((nt - 1,)),
        ],
        compiler_params=pltpu.CompilerParams(
            collective_id=0, has_side_effects=True, vmem_limit_bytes=VMEM_BYTES - tail
        ),
    )(
        cond[None], ctx_cond[None], norm_gain[None], table, latents, context, shift_weight, scale_weight, gate_weight,
        q_weight, k_weight, v_weight, out_weight,
    )
    return pl.pallas_call(
        finish,
        out_shape=jax.ShapeDtypeStruct((own_n, d), BF16),
        in_specs=[vmem] * 5,
        out_specs=hbm,
        scratch_shapes=[pltpu.VMEM((own_n, d), BF16), sem((4,))],
        compiler_params=pltpu.CompilerParams(vmem_limit_bytes=16 * 1024 * 1024),
    )(*parts)


def solution(mesh):
    in_specs = (
        P("sp", None),
        P(),
        P(),
        P("sp", None),
        P(),
        P("tp", None),
        P("tp", None),
        P("tp", None),
        P(None, "tp"),
        P(None, "tp"),
        P(None, "tp"),
        P(),
        P("tp", None, None),
    )
    body = functools.partial(shards, mesh.shape["sp"], mesh.shape["tp"])
    return jax.shard_map(
        body, mesh=mesh, in_specs=in_specs, out_specs=P(("sp", "tp"), None), check_vma=False
    )
```
